32 devices in a mesh: fs: 16 (over z, x, core), tp: 2 (over y).
Axes of the slice: x: 2, y: 2, z: 4, core: 2. Of those that a mesh axis runs over, the one named last changes fastest.
Arguments:
- normed_input: bfloat16 [8192, 2048], P('fs'), may hold values from -6 to 6
- value_cotangent: bfloat16 [8192, 2048], P('fs', 'tp'), may hold values from -6 to 6
- gated_output: bfloat16 [8192, 2048], P('fs', 'tp'), may hold values from -6 to 6
- layer_cotangent: bfloat16 [8192, 2048], P('fs'), may hold values from -6 to 6
- factor_value: bfloat16 [2048, 256], P('fs'), may hold values from -4 to 4, as said below
- factor_output: bfloat16 [2048, 256], P('fs'), may hold values from -4 to 4, as said below
- weight_value: float32 [2048, 2048], P('fs', 'tp'), may hold values from -0.125 to 0.125
- weight_output: float32 [2048, 2048], P('tp', 'fs'), may hold values from -0.125 to 0.125
- first_value: float32 [256, 2048], P('fs', 'tp'), may hold values from -2048 to 2048
- second_value: float32 [256, 2048], P('fs', 'tp'), may hold values from 32768 to 524288
- first_output: float32 [256, 2048], P('fs', 'tp'), may hold values from -2048 to 2048
- second_output: float32 [256, 2048], P('fs', 'tp'), may hold values from 32768 to 524288
Outputs:
- step_value: float32 [2048, 2048], P('fs', 'tp')
- step_output: float32 [2048, 2048], P('tp', 'fs')
- next_weight_value: float32 [2048, 2048], P('fs', 'tp')
- next_weight_output: float32 [2048, 2048], P('tp', 'fs')
- next_first_value: float32 [256, 2048], P('fs', 'tp')
- next_second_value: float32 [256, 2048], P('fs', 'tp')
- next_first_output: float32 [256, 2048], P('fs', 'tp')
- next_second_output: float32 [256, 2048], P('fs', 'tp')
- copy_value: bfloat16 [2048, 2048], P(None, 'tp')
- copy_output: bfloat16 [2048, 2048], P('tp')
The draws below stay inside these ranges and needn't reach their ends.
Inputs may be any that keep to these rules, and one draw needn't show every extreme that they name: factor_value has full rank. factor_output has full rank.
All inputs are finite; a program needn't handle non-finite values.
Results may differ from the reference program's by a relative error of at most 0.0039.
Values may be sent and summed in bfloat16 or wider, within the bound.
A program may use at most 64 MiB of HBM per device.

```python
import math
import jax
import jax.numpy as jnp
from jax import lax

D = 2048
WIDTH = 2048
R = 256
TOKENS = 8192


def make_factor(key):
    rising = jnp.exp(jnp.log(10.0) * jnp.arange(D, dtype=jnp.float32) / D)
    base = jnp.clip(jax.random.normal(key, (D, R), jnp.float32), -6.0, 6.0)
    return (base * rising[:, None] / jnp.sqrt(jnp.float32(D))).astype(jnp.bfloat16)


def draw_factor_value(key, part):
    return make_factor(jax.random.fold_in(key, 11))


def draw_factor_output(key, part):
    return make_factor(jax.random.fold_in(key, 17))


def shard_levels(key, dims, split, low, high):
    gain, own = 1.0, jax.random.fold_in(key, 6)
    for position, parts in split:
        heights = jnp.exp(jax.random.uniform(jax.random.fold_in(own, position), (parts,), jnp.float32, low / len(split), high / len(split)))
        gain = gain * jnp.repeat(heights, dims[position] // parts).reshape([-1 if axis == position else 1 for axis in range(len(dims))])
    return gain


def scatter_about(own_key, shape, scale, limit, pieces=(), held_as=jnp.bfloat16):
    array = scale * jax.random.normal(own_key, shape, jnp.float32)
    if pieces:
        array = array * shard_levels(own_key, shape, pieces, -0.22, 0.18)
    return jnp.clip(array, -limit, limit).astype(held_as)


def setup_inputs(seed: int = 0) -> dict:
    keys = jax.random.split(jax.random.key(seed), 13)
    normed_input = scatter_about(keys[0], (TOKENS, D), 1.0, 6.0, ((0, 16),))
    value_cotangent = scatter_about(keys[1], (TOKENS, WIDTH), 1.0, 6.0, ((0, 16), (1, 2)))
    gated_output = scatter_about(keys[2], (TOKENS, WIDTH), 1.0, 6.0, ((0, 16), (1, 2)))
    layer_cotangent = scatter_about(keys[3], (TOKENS, D), 1.0, 6.0, ((0, 16),))
    factor_value = draw_factor_value(jax.random.fold_in(keys[12], 71), 0)
    factor_output = draw_factor_output(jax.random.fold_in(keys[12], 71), 0)
    weight_value = scatter_about(keys[6], (D, WIDTH), D ** -0.5, 0.125, ((0, 16), (1, 2)), jnp.float32)
    weight_output = scatter_about(keys[7], (WIDTH, D), WIDTH ** -0.5, 0.125, ((0, 2), (1, 16)), jnp.float32)
    first_value = scatter_about(keys[8], (R, WIDTH), (4 * TOKENS ** 0.5), 2048.0, ((0, 16), (1, 2)), jnp.float32)
    second_value = jnp.clip(jnp.exp(math.log(524288.0) - 2.7725887 * jax.random.uniform(keys[9], (R, WIDTH), jnp.float32) ** shard_levels(keys[9], (R, WIDTH), ((0, 16), (1, 2)), -0.2, 0.2)), 32768.0, 524288.0)
    first_output = scatter_about(keys[10], (R, WIDTH), (4 * TOKENS ** 0.5), 2048.0, ((0, 16), (1, 2)), jnp.float32)
    second_output = jnp.clip(jnp.exp(math.log(524288.0) - 2.7725887 * jax.random.uniform(keys[11], (R, WIDTH), jnp.float32) ** shard_levels(keys[11], (R, WIDTH), ((0, 16), (1, 2)), -0.2, 0.2)), 32768.0, 524288.0)
    return dict(normed_input=normed_input, value_cotangent=value_cotangent, gated_output=gated_output, layer_cotangent=layer_cotangent, factor_value=factor_value, factor_output=factor_output, weight_value=weight_value, weight_output=weight_output, first_value=first_value, second_value=second_value, first_output=first_output, second_output=second_output)


def reference(normed_input, value_cotangent, gated_output, layer_cotangent, factor_value, factor_output, weight_value, weight_output, first_value, second_value, first_output, second_output):
    projected_input = jnp.dot(normed_input, factor_value, preferred_element_type=jnp.float32).astype(jnp.bfloat16)
    projected_cotangent = jnp.dot(layer_cotangent, factor_output, preferred_element_type=jnp.float32).astype(jnp.bfloat16)
    low_value = jnp.dot(projected_input.T, value_cotangent, preferred_element_type=jnp.float32)
    low_output = jnp.dot(projected_cotangent.T, gated_output, preferred_element_type=jnp.float32)
    next_first_value = 0.9 * first_value + 0.1 * low_value
    next_second_value = 0.95 * second_value + 0.05 * low_value * low_value
    next_first_output = 0.9 * first_output + 0.1 * low_output
    next_second_output = 0.95 * second_output + 0.05 * low_output * low_output
    direction_value = (next_first_value * lax.rsqrt(next_second_value)).astype(jnp.bfloat16)
    direction_output = (next_first_output * lax.rsqrt(next_second_output)).astype(jnp.bfloat16)
    update_value = jnp.dot(factor_value, direction_value, preferred_element_type=jnp.float32)
    update_output = jnp.dot(direction_output.T, factor_output.T, preferred_element_type=jnp.float32)
    entries = D * WIDTH
    total_value = jnp.sum(update_value * update_value)
    total_output = jnp.sum(update_output * update_output)
    step_value = update_value * lax.rsqrt(total_value / entries + 1e-06)
    step_output = update_output * lax.rsqrt(total_output / entries + 1e-06)
    next_weight_value = weight_value - 0.02 * step_value
    next_weight_output = weight_output - 0.02 * step_output
    return (step_value, step_output, next_weight_value, next_weight_output, next_first_value, next_second_value, next_first_output, next_second_output, next_weight_value.astype(jnp.bfloat16), next_weight_output.astype(jnp.bfloat16))
```

```python
import functools

import jax
import jax.numpy as jnp
from jax import lax
from jax.experimental import pallas as pl
from jax.experimental.pallas import tpu as pltpu
from jax.sharding import PartitionSpec as P

CORES = 2

D = 2048
WIDTH = 2048


def gram_times(gram_matrix, directions):
    gram_high = gram_matrix.astype(jnp.bfloat16)
    gram_low = (gram_matrix - gram_high.astype(jnp.float32)).astype(jnp.bfloat16)
    return jnp.dot(gram_high, directions, preferred_element_type=jnp.float32) + jnp.dot(
        gram_low, directions, preferred_element_type=jnp.float32
    )


def body(
    normed_input,
    value_cotangent,
    gated_output,
    layer_cotangent,
    factor_value,
    factor_output,
    weight_value,
    weight_output,
    first_value,
    second_value,
    first_output,
    second_output,
):
    col_count = value_cotangent.shape[1]
    inner = (((0,), (0,)), ((), ()))
    pieces = (
        lax.all_gather(factor_value, "fs", axis=0, tiled=True),
        lax.all_gather(factor_output, "fs", axis=0, tiled=True),
    )
    piece_value, piece_output = pieces
    span_input = normed_input
    span_cotan = layer_cotangent
    gram_value = lax.dot_general(pieces[0], pieces[0], inner, preferred_element_type=jnp.float32)
    gram_output = lax.dot_general(pieces[1], pieces[1], inner, preferred_element_type=jnp.float32)
    projected_input = jnp.dot(span_input, piece_value, preferred_element_type=jnp.float32).astype(
        jnp.bfloat16
    )
    projected_cotangent = jnp.dot(
        span_cotan, piece_output, preferred_element_type=jnp.float32
    ).astype(jnp.bfloat16)
    span_input = projected_input
    span_cotan = projected_cotangent
    term_value = lax.dot_general(
        span_input, value_cotangent, inner, preferred_element_type=jnp.float32
    )
    term_output = lax.dot_general(
        span_cotan, gated_output, inner, preferred_element_type=jnp.float32
    )
    low_rank = lax.psum_scatter(
        jnp.concatenate([term_value, term_output], axis=1), "fs", scatter_dimension=0, tiled=True
    )
    low_value = low_rank[:, :col_count]
    low_output = low_rank[:, col_count:]
    next_first_value = 0.9 * first_value + 0.1 * low_value
    next_second_value = 0.95 * second_value + 0.05 * low_value * low_value
    next_first_output = 0.9 * first_output + 0.1 * low_output
    next_second_output = 0.95 * second_output + 0.05 * low_output * low_output
    direction_value = (next_first_value * lax.rsqrt(next_second_value)).astype(jnp.bfloat16)
    direction_output = (next_first_output * lax.rsqrt(next_second_output)).astype(jnp.bfloat16)
    gathered_value, gathered_output = (
        lax.all_gather(direction_value, "fs", axis=0, tiled=True),
        lax.all_gather(direction_output, "fs", axis=0, tiled=True),
    )
    update_value = jnp.dot(factor_value, gathered_value, preferred_element_type=jnp.float32)
    update_output = lax.dot_general(
        gathered_output, factor_output, (((0,), (1,)), ((), ())), preferred_element_type=jnp.float32
    )
    square_value = jnp.sum(
        gathered_value.astype(jnp.float32) * gram_times(gram_value, gathered_value)
    )
    square_output = jnp.sum(
        gathered_output.astype(jnp.float32) * gram_times(gram_output, gathered_output)
    )
    total_value, total_output = lax.psum((square_value, square_output), "tp")
    entries = D * WIDTH
    step_value = update_value * lax.rsqrt(total_value / entries + 1e-06)
    step_output = update_output * lax.rsqrt(total_output / entries + 1e-06)
    next_weight_value = weight_value - 0.02 * step_value
    next_weight_output = weight_output - 0.02 * step_output
    half_value = next_weight_value.astype(jnp.bfloat16)
    half_output = next_weight_output.astype(jnp.bfloat16)
    copy_value, copy_output = (
        lax.all_gather(half_value, "fs", axis=0, tiled=True),
        lax.all_gather(half_output, "fs", axis=1, tiled=True),
    )
    return (
        step_value,
        step_output,
        next_weight_value,
        next_weight_output,
        next_first_value,
        next_second_value,
        next_first_output,
        next_second_output,
        copy_value,
        copy_output,
    )


def next_moments(first, second, low):
    return 0.9 * first + 0.1 * low, 0.95 * second + 0.05 * low * low


MESH = pl.DeviceIdType.MESH


class Sender:
    def __init__(self, sems):
        self.sems, self.pending = sems, []

    def send(self, source, target, recv_sem, device, when=None):
        copy = pltpu.make_async_remote_copy(
            src_ref=source,
            dst_ref=target,
            send_sem=self.sems.at[len(self.pending)],
            recv_sem=recv_sem,
            device_id=device,
            device_id_type=MESH,
        )
        self.guarded(copy.start, when)
        self.pending.append((copy, when))

    def guarded(self, action, when):
        if when is None:
            action()
        else:

            @pl.when(when)
            def _():
                action()

    def drain(self):
        for copy, when in self.pending:
            self.guarded(copy.wait_send, when)


def fused(
    fs_size,
    tp_size,
    input_hbm,
    value_hbm,
    gated_hbm,
    layer_hbm,
    factor_value_hbm,
    factor_output_hbm,
    weight_value_hbm,
    weight_output_hbm,
    first_value_hbm,
    second_value_hbm,
    first_output_hbm,
    second_output_hbm,
    moments,
    directions,
    turned,
    factors,
    scale_ref,
    wide_value,
    wide_output,
    stream,
    cotan,
    weight_value,
    weight_output,
    old,
    projection,
    flipped,
    terms,
    paired,
    out_x,
    in_x,
    out_z,
    in_z,
    totals,
    load_sem,
    send_sem,
    factor_recv,
    weight_recv,
    direction_recv,
    pair_recv,
    x_recv,
    z_recv,
    total_recv,
):
    fs, tp = lax.axis_index("fs"), lax.axis_index("tp")
    width = tp_size
    chips = fs_size // CORES
    depth = chips // width
    core, chip = lax.rem(fs, CORES), fs // CORES
    x, z = lax.rem(chip, width), chip // width
    rows, rank = factor_value_hbm.shape
    tokens = input_hbm.shape[0]
    cols = value_hbm.shape[1]
    ranks = first_value_hbm.shape[0]
    model = rows * fs_size
    last = depth - 1
    span = CORES * rows

    def index(z_at, x_at, core_at):
        return (z_at * width + x_at) * CORES + core_at

    def along_z(z_at):
        return {"fs": index(z_at, x, core)}

    over_x = {"fs": index(z, 1 - x, core)}
    over_core = {"fs": index(z, x, 1 - core)}
    over_y = {"tp": 1 - tp}
    beside = z + 1 - 2 * lax.rem(z, 2)
    mirror = last - z
    across = lax.rem(z + depth // 2, depth)
    others = (beside, mirror, across)
    middle = jnp.logical_and(z > 0, z < last)

    def block(ref, origin, size):
        return ref.at[pl.ds(pl.multiple_of(origin * size, size), size)]

    sources = (
        factor_value_hbm,
        factor_output_hbm,
        weight_value_hbm,
        weight_output_hbm,
        input_hbm,
        layer_hbm,
        value_hbm,
        gated_hbm,
        first_value_hbm,
        second_value_hbm,
        first_output_hbm,
        second_output_hbm,
    )
    targets = (
        block(factors.at[0], fs, rows),
        block(factors.at[1], fs, rows),
        weight_value,
        weight_output,
        stream.at[0],
        stream.at[1],
        cotan.at[0],
        cotan.at[1],
        old.at[0],
        old.at[1],
        old.at[2],
        old.at[3],
    )
    loads = [
        pltpu.make_async_copy(source, target, load_sem.at[slot])
        for slot, (source, target) in enumerate(zip(sources, targets))
    ]
    for load in loads:
        load.start()

    barrier = pltpu.get_barrier_semaphore()
    peers = [along_z(z_at) for z_at in others] + [over_x, over_core, over_y]
    for peer in peers:
        pl.semaphore_signal(barrier, inc=1, device_id=peer, device_id_type=MESH)
    loads[0].wait()
    loads[1].wait()
    pl.semaphore_wait(barrier, len(peers))

    sender = Sender(send_sem)

    def arrived(ref, recv_sem):
        pltpu.make_async_remote_copy(
            src_ref=ref,
            dst_ref=ref,
            send_sem=send_sem.at[0],
            recv_sem=recv_sem,
            device_id=over_core,
            device_id_type=MESH,
        ).wait_recv()

    def forward(ref, recv_sem, device, when=None):
        sender.send(ref, ref, recv_sem, device, when)

    mine, theirs = tp, 1 - tp

    def factor(kind, origin):
        return block(factors.at[kind], origin, rows), factor_recv.at[kind, origin]

    for z_at in others:
        forward(*factor(mine, fs), along_z(z_at))
    forward(*factor(mine, fs), over_x)
    forward(*factor(theirs, fs), over_x)
    forward(*factor(mine, fs), over_core)
    forward(*factor(theirs, fs), over_core)

    half_rows, half_cols = rows // 2, cols // 2

    def piece(part, origin):
        start = pl.multiple_of(origin * rows, rows)
        if part < 2:
            ref = wide_value.at[pl.ds(start + part * half_rows, half_rows)]
        else:
            ref = wide_output.at[pl.ds((part - 2) * half_cols, half_cols), pl.ds(start, rows)]
        return ref, weight_recv.at[part, origin]

    def piece_z(part, origin):
        forward(*piece(part, origin), along_z(beside))
        forward(*piece(part, origin), along_z(mirror), middle)
        forward(*piece(part, origin), along_z(across))

    beyond = along_z(jnp.clip(last * (z - 1), 0, last))

    def piece_arrives_z(part, x_at, cross):
        for z_at in others:
            ref, sem = piece(part, index(z_at, x_at, core))
            arrived(ref, sem)
            if z_at is across:
                forward(ref, sem, beyond, middle)
            if cross:
                forward(ref, sem, over_x)
            forward(ref, sem, over_core)

    def piece_arrives_x(part, z_at):
        ref, sem = piece(part, index(z_at, 1 - x, core))
        arrived(ref, sem)
        forward(ref, sem, over_core)

    loads[2].wait()
    loads[3].wait()
    own_rows = pl.ds(pl.multiple_of(fs * rows, rows), rows)
    wide_value[own_rows, :] = weight_value[...].astype(jnp.bfloat16)
    wide_output[:, own_rows] = weight_output[...].astype(jnp.bfloat16)
    piece_z(1, fs)
    piece_z(2, fs)

    for z_at in others:
        ref, sem = factor(mine, index(z_at, x, core))
        arrived(ref, sem)
        forward(ref, sem, over_x)
        forward(ref, sem, over_y)
        forward(ref, sem, over_core)
    for part in range(4):
        forward(*piece(part, fs), over_x)
    ref, sem = factor(theirs, index(z, 1 - x, core))
    arrived(ref, sem)
    forward(ref, sem, over_core)
    for z_at in (z,) + others:
        ref, sem = factor(mine, index(z_at, 1 - x, core))
        arrived(ref, sem)
        if z_at is not z:
            forward(ref, sem, over_y)
        forward(ref, sem, over_core)
    for load in loads[4:]:
        load.wait()

    def project(kind, z_at, x_at, first=False):
        arrived(*factor(kind, index(z_at, x_at, 1 - core)))
        part = pl.ds(pl.multiple_of((z_at * width + x_at) * span, span), span)
        product = jnp.dot(
            stream[kind, :, part], factors[kind, part], preferred_element_type=jnp.float32
        )
        projection[kind] = product if first else projection[kind] + product

    def from_y(z_at, x_at):
        ref, sem = factor(theirs, index(z_at, x_at, core))
        arrived(ref, sem)
        forward(ref, sem, over_core)

    project(mine, z, x, True)
    project(theirs, z, x, True)
    for z_at in others:
        project(mine, z_at, x)
    for z_at in others:
        from_y(z_at, x)
    for z_at in (z,) + others:
        project(mine, z_at, 1 - x)
    for z_at in others:
        from_y(z_at, 1 - x)
    for part in range(4):
        forward(*piece(part, fs), over_core)
    for z_at in others:
        project(theirs, z_at, x)
    for z_at in (z,) + others:
        project(theirs, z_at, 1 - x)

    width_tile = 256
    for kind in range(2):
        flipped[...] = projection[kind].T.astype(jnp.bfloat16)

        @pl.loop(0, cols // width_tile)
        def _(step, kind=kind):
            tile = pl.ds(pl.multiple_of(step * width_tile, width_tile), width_tile)
            term = jnp.dot(flipped[...], cotan[kind, :, tile], preferred_element_type=jnp.float32)
            target = pl.ds(pl.multiple_of(kind * cols + step * width_tile, width_tile), width_tile)
            terms[:, :, :, target] = term.reshape(chips, CORES, ranks, width_tile)

    far = others + (z,)
    for x_at in (1 - x, x):
        for z_at in far:
            to = z_at * width + x_at
            sender.send(terms.at[to, 1 - core], paired.at[to], pair_recv.at[to], over_core)

    def pair_sum(z_at, x_at):
        at = z_at * width + x_at
        arrived(paired.at[at], pair_recv.at[at])
        return terms[at, core] + paired[at]

    for z_at in far:
        out_x[z_at] = pair_sum(z_at, 1 - x).astype(jnp.bfloat16)
        sender.send(out_x.at[z_at], in_x.at[z_at], x_recv.at[z_at], over_x)
    piece_arrives_z(1, x, True)

    def column_sum(z_at):
        total = pair_sum(z_at, x)
        arrived(in_x.at[z_at], x_recv.at[z_at])
        return total + in_x[z_at].astype(jnp.float32)

    for z_at in others:
        out_z[z_at] = column_sum(z_at).astype(jnp.bfloat16)
        sender.send(out_z.at[z_at], in_z.at[z], z_recv.at[z], along_z(z_at))
    piece_z(3, fs)
    low = column_sum(z)
    for z_at in others:
        arrived(in_z.at[z_at], z_recv.at[z_at])
        low = low + in_z[z_at].astype(jnp.float32)

    own_ranks = pl.ds(pl.multiple_of(fs * ranks, ranks), ranks)
    for kind in range(2):
        part = low[:, kind * cols : (kind + 1) * cols]
        next_first, next_second = next_moments(old[2 * kind], old[2 * kind + 1], part)
        moments[2 * kind] = next_first
        moments[2 * kind + 1] = next_second
        directions[own_ranks, kind * cols : (kind + 1) * cols] = (
            next_first * lax.rsqrt(next_second)
        ).astype(jnp.bfloat16)

    def direction(origin):
        return block(directions, origin, ranks), direction_recv.at[origin]

    for z_at in others:
        forward(*direction(fs), along_z(z_at))
    forward(*direction(fs), over_x)
    forward(*direction(fs), over_core)
    for z_at in others:
        ref, sem = direction(index(z_at, x, core))
        arrived(ref, sem)
        forward(ref, sem, over_x)
        forward(ref, sem, over_core)
    piece_arrives_x(0, z)
    piece_z(0, fs)
    piece_z(0, index(z, 1 - x, core))
    piece_arrives_z(2, x, True)
    for z_at in (z,) + others:
        ref, sem = direction(index(z_at, 1 - x, core))
        arrived(ref, sem)
        forward(ref, sem, over_core)
    for z_at in (z,) + others:
        for x_at in (x, 1 - x):
            arrived(*direction(index(z_at, x_at, 1 - core)))

    tile = 256
    for kind in range(2):
        totals[tp, kind] = jnp.zeros((8, cols), jnp.float32)

        @pl.loop(0, model // tile)
        def _(step, kind=kind):
            update = jnp.dot(
                factors[kind, pl.ds(pl.multiple_of(step * tile, tile), tile)],
                directions[:, kind * cols : (kind + 1) * cols],
                preferred_element_type=jnp.float32,
            )
            totals[tp, kind] += jnp.sum((update * update).reshape(tile // 8, 8, cols), axis=0)

    sender.send(totals.at[tp], totals.at[tp], total_recv.at[tp], over_y)
    turned[...] = directions[:, cols:].astype(jnp.float32).T.astype(jnp.bfloat16)

    piece_arrives_z(3, x, True)
    for z_at in (z,) + others:
        piece_arrives_x(1, z_at)
    piece_arrives_z(0, x, False)
    piece_arrives_z(0, 1 - x, False)
    arrived(totals.at[1 - tp], total_recv.at[1 - tp])
    entries = model * cols * tp_size
    for kind in range(2):
        total = jnp.sum(totals[0, kind] + totals[1, kind], keepdims=True)
        scale = lax.rsqrt(total / entries + 1e-06)
        scale_ref[kind] = jnp.broadcast_to(scale, scale_ref.shape[1:])
    for part in (2, 3):
        for z_at in (z,) + others:
            piece_arrives_x(part, z_at)
    for part in range(4):
        for z_at in (z,) + others:
            for x_at in (x, 1 - x):
                arrived(*piece(part, index(z_at, x_at, 1 - core)))
    sender.drain()


def apply(
    moments,
    directions,
    turned,
    factors,
    scale_ref,
    wide_value,
    wide_output,
    weight_value_hbm,
    weight_output_hbm,
    step_value_hbm,
    step_output_hbm,
    next_weight_value_hbm,
    next_weight_output_hbm,
    next_first_value_hbm,
    next_second_value_hbm,
    next_first_output_hbm,
    next_second_output_hbm,
    copy_value_hbm,
    copy_output_hbm,
    weight_value,
    weight_output,
    step_value,
    step_output,
    next_value,
    next_output,
    copy_value,
    copy_output,
    load_sem,
    store_sem,
    value_sem,
    output_sem,
):
    rows, cols = weight_value_hbm.shape
    model = factors.shape[1]
    fs = lax.axis_index("fs")
    scale_value, scale_output = scale_ref[0, :1, :1], scale_ref[1, :1, :1]
    transposed = (((1,), (1,)), ((), ()))
    loads = [
        pltpu.make_async_copy(weight_value_hbm, weight_value, load_sem.at[0]),
        pltpu.make_async_copy(weight_output_hbm, weight_output, load_sem.at[1]),
    ]
    for load in loads:
        load.start()
    stores = []

    def store(source, target):
        copy = pltpu.make_async_copy(source, target, store_sem.at[len(stores)])
        copy.start()
        stores.append(copy)

    store(moments.at[0], next_first_value_hbm)
    store(moments.at[1], next_second_value_hbm)
    store(moments.at[2], next_first_output_hbm)
    store(moments.at[3], next_second_output_hbm)

    def update_value(factor):
        return jnp.dot(factor, directions[:, :cols], preferred_element_type=jnp.float32)

    def update_output(factor):
        return lax.dot_general(turned[...], factor, transposed, preferred_element_type=jnp.float32)

    tile = 256

    def value_copy(step):
        part = pl.ds(pl.multiple_of(step * tile, tile), tile)
        return pltpu.make_async_copy(
            copy_value.at[part], copy_value_hbm.at[part], value_sem.at[step]
        )

    def output_copy(step):
        part = pl.ds(pl.multiple_of(step * tile, tile), tile)
        return pltpu.make_async_copy(
            copy_output.at[:, part], copy_output_hbm.at[:, part], output_sem.at[step]
        )

    @pl.loop(0, model // tile)
    def _(step):
        part = pl.ds(pl.multiple_of(step * tile, tile), tile)
        copy_value[part] = (
            wide_value[part].astype(jnp.float32)
            - update_value(factors[0, part]) * (0.02 * scale_value)
        ).astype(jnp.bfloat16)
        value_copy(step).start()

    own_rows = pl.ds(pl.multiple_of(fs * rows, rows), rows)
    loads[0].wait()
    step = update_value(factors[0, own_rows]) * scale_value
    step_value[...] = step
    store(step_value, step_value_hbm)
    next_value[...] = weight_value[...] - 0.02 * step
    store(next_value, next_weight_value_hbm)
    loads[1].wait()
    step = update_output(factors[1, own_rows]) * scale_output
    step_output[...] = step
    store(step_output, step_output_hbm)
    next_output[...] = weight_output[...] - 0.02 * step
    store(next_output, next_weight_output_hbm)

    @pl.loop(0, model // tile)
    def _(step):
        part = pl.ds(pl.multiple_of(step * tile, tile), tile)
        copy_output[:, part] = (
            wide_output[:, part].astype(jnp.float32)
            - update_output(factors[1, part]) * (0.02 * scale_output)
        ).astype(jnp.bfloat16)
        output_copy(step).start()

    for copy in stores:
        copy.wait()
    for step in range(model // tile):
        value_copy(step).wait()
        output_copy(step).wait()


def fused_body(fs_size, tp_size, *args):
    tokens, model = args[0].shape
    cols = args[1].shape[1]
    rows, rank = args[4].shape
    ranks = args[8].shape[0]
    chips = fs_size // CORES
    depth = chips // tp_size
    f32, bf16 = jnp.float32, jnp.bfloat16
    vmem = pl.BlockSpec(memory_space=pltpu.VMEM)
    hbm = pl.BlockSpec(memory_space=pltpu.HBM)
    shape = jax.ShapeDtypeStruct
    dma = pltpu.SemaphoreType.DMA
    args = [pltpu.with_memory_space_constraint(arg, pltpu.HBM) for arg in args]
    gathered = pl.pallas_call(
        functools.partial(fused, fs_size, tp_size),
        out_shape=[
            shape((4, ranks, cols), f32),
            shape((rank, 2 * cols), bf16),
            shape((cols, rank), bf16),
            shape((2, model, rank), bf16),
            shape((2, 8, 128), f32),
            shape((model, cols), bf16),
            shape((cols, model), bf16),
        ],
        in_specs=[hbm] * 12,
        out_specs=[vmem] * 7,
        scratch_shapes=[
            pltpu.VMEM((2, tokens, model), bf16),
            pltpu.VMEM((2, tokens, cols), bf16),
            pltpu.VMEM((rows, cols), f32),
            pltpu.VMEM((cols, rows), f32),
            pltpu.VMEM((4, ranks, cols), f32),
            pltpu.VMEM((2, tokens, rank), f32),
            pltpu.VMEM((rank, tokens), bf16),
            pltpu.VMEM((chips, CORES, ranks, 2 * cols), f32),
            pltpu.VMEM((chips, ranks, 2 * cols), f32),
        ]
        + [pltpu.VMEM((depth, ranks, 2 * cols), bf16)] * 4
        + [
            pltpu.VMEM((tp_size, 2, 8, cols), f32),
            dma((12,)),
            dma((192,)),
            dma((2, fs_size)),
            dma((4, fs_size)),
            dma((fs_size,)),
            dma((chips,)),
            dma((depth,)),
            dma((depth,)),
            dma((tp_size,)),
        ],
        compiler_params=pltpu.CompilerParams(
            collective_id=0, has_side_effects=True, vmem_limit_bytes=24 * 1024 * 1024
        ),
    )(*args)

    steps = model // 256
    return pl.pallas_call(
        apply,
        out_shape=[shape((rows, cols), f32), shape((cols, rows), f32)] * 2
        + [shape((ranks, cols), f32)] * 4
        + [shape((model, cols), bf16), shape((cols, model), bf16)],
        in_specs=[vmem] * 7 + [hbm] * 2,
        out_specs=[hbm] * 10,
        scratch_shapes=[pltpu.VMEM((rows, cols), f32), pltpu.VMEM((cols, rows), f32)] * 3
        + [
            pltpu.VMEM((model, cols), bf16),
            pltpu.VMEM((cols, model), bf16),
            dma((2,)),
            dma((8,)),
            dma((steps,)),
            dma((steps,)),
        ],
        compiler_params=pltpu.CompilerParams(vmem_limit_bytes=24 * 1024 * 1024),
    )(*gathered, *args[6:8])


def solution(mesh):
    fs_size, tp_size = mesh.shape["fs"], mesh.shape["tp"]
    placed = (
        P("fs", None),
        P("fs", "tp"),
        P("fs", "tp"),
        P("fs", None),
        P("fs", None),
        P("fs", None),
        P("fs", "tp"),
        P("tp", "fs"),
        P("fs", "tp"),
        P("fs", "tp"),
        P("fs", "tp"),
        P("fs", "tp"),
    )
    chips = fs_size // CORES
    tiled = tp_size == 2 and fs_size == 16 and chips % tp_size == 0
    return jax.shard_map(
        functools.partial(fused_body, fs_size, tp_size) if tiled else body,
        mesh=mesh,
        in_specs=placed,
        out_specs=(
            P("fs", "tp"),
            P("tp", "fs"),
            P("fs", "tp"),
            P("tp", "fs"),
            P("fs", "tp"),
            P("fs", "tp"),
            P("fs", "tp"),
            P("fs", "tp"),
            P(None, "tp"),
            P("tp", None),
        ),
        check_vma=False,
    )
```

```python
import functools

import jax
import jax.numpy as jnp
from jax import lax
from jax.experimental import pallas as pl
from jax.experimental.pallas import tpu as pltpu
from jax.sharding import PartitionSpec as P

CORES = 2

D = 2048
WIDTH = 2048


def gram_times(gram_matrix, directions):
    gram_high = gram_matrix.astype(jnp.bfloat16)
    gram_low = (gram_matrix - gram_high.astype(jnp.float32)).astype(jnp.bfloat16)
    return jnp.dot(gram_high, directions, preferred_element_type=jnp.float32) + jnp.dot(
        gram_low, directions, preferred_element_type=jnp.float32
    )


def body(
    normed_input,
    value_cotangent,
    gated_output,
    layer_cotangent,
    factor_value,
    factor_output,
    weight_value,
    weight_output,
    first_value,
    second_value,
    first_output,
    second_output,
):
    col_count = value_cotangent.shape[1]
    inner = (((0,), (0,)), ((), ()))
    pieces = (
        lax.all_gather(factor_value, "fs", axis=0, tiled=True),
        lax.all_gather(factor_output, "fs", axis=0, tiled=True),
    )
    piece_value, piece_output = pieces
    span_input = normed_input
    span_cotan = layer_cotangent
    gram_value = lax.dot_general(pieces[0], pieces[0], inner, preferred_element_type=jnp.float32)
    gram_output = lax.dot_general(pieces[1], pieces[1], inner, preferred_element_type=jnp.float32)
    projected_input = jnp.dot(span_input, piece_value, preferred_element_type=jnp.float32).astype(
        jnp.bfloat16
    )
    projected_cotangent = jnp.dot(
        span_cotan, piece_output, preferred_element_type=jnp.float32
    ).astype(jnp.bfloat16)
    span_input = projected_input
    span_cotan = projected_cotangent
    term_value = lax.dot_general(
        span_input, value_cotangent, inner, preferred_element_type=jnp.float32
    )
    term_output = lax.dot_general(
        span_cotan, gated_output, inner, preferred_element_type=jnp.float32
    )
    low_rank = lax.psum_scatter(
        jnp.concatenate([term_value, term_output], axis=1), "fs", scatter_dimension=0, tiled=True
    )
    low_value = low_rank[:, :col_count]
    low_output = low_rank[:, col_count:]
    next_first_value = 0.9 * first_value + 0.1 * low_value
    next_second_value = 0.95 * second_value + 0.05 * low_value * low_value
    next_first_output = 0.9 * first_output + 0.1 * low_output
    next_second_output = 0.95 * second_output + 0.05 * low_output * low_output
    direction_value = (next_first_value * lax.rsqrt(next_second_value)).astype(jnp.bfloat16)
    direction_output = (next_first_output * lax.rsqrt(next_second_output)).astype(jnp.bfloat16)
    gathered_value, gathered_output = (
        lax.all_gather(direction_value, "fs", axis=0, tiled=True),
        lax.all_gather(direction_output, "fs", axis=0, tiled=True),
    )
    update_value = jnp.dot(factor_value, gathered_value, preferred_element_type=jnp.float32)
    update_output = lax.dot_general(
        gathered_output, factor_output, (((0,), (1,)), ((), ())), preferred_element_type=jnp.float32
    )
    square_value = jnp.sum(
        gathered_value.astype(jnp.float32) * gram_times(gram_value, gathered_value)
    )
    square_output = jnp.sum(
        gathered_output.astype(jnp.float32) * gram_times(gram_output, gathered_output)
    )
    total_value, total_output = lax.psum((square_value, square_output), "tp")
    entries = D * WIDTH
    step_value = update_value * lax.rsqrt(total_value / entries + 1e-06)
    step_output = update_output * lax.rsqrt(total_output / entries + 1e-06)
    next_weight_value = weight_value - 0.02 * step_value
    next_weight_output = weight_output - 0.02 * step_output
    half_value = next_weight_value.astype(jnp.bfloat16)
    half_output = next_weight_output.astype(jnp.bfloat16)
    copy_value, copy_output = (
        lax.all_gather(half_value, "fs", axis=0, tiled=True),
        lax.all_gather(half_output, "fs", axis=1, tiled=True),
    )
    return (
        step_value,
        step_output,
        next_weight_value,
        next_weight_output,
        next_first_value,
        next_second_value,
        next_first_output,
        next_second_output,
        copy_value,
        copy_output,
    )


def next_moments(first, second, low):
    return 0.9 * first + 0.1 * low, 0.95 * second + 0.05 * low * low


MESH = pl.DeviceIdType.MESH


class Sender:
    def __init__(self, sems):
        self.sems, self.pending, self.drained = sems, [], 0

    def send(self, source, target, recv_sem, device, when=None):
        copy = pltpu.make_async_remote_copy(
            src_ref=source,
            dst_ref=target,
            send_sem=self.sems.at[len(self.pending)],
            recv_sem=recv_sem,
            device_id=device,
            device_id_type=MESH,
        )
        self.guarded(copy.start, when)
        self.pending.append((copy, when))

    def guarded(self, action, when):
        if when is None:
            action()
        else:

            @pl.when(when)
            def _():
                action()

    def drain(self, count=None):
        count = len(self.pending) if count is None else count
        for copy, when in self.pending[self.drained : count]:
            self.guarded(copy.wait_send, when)
        self.drained = count


def fused(
    fs_size,
    tp_size,
    input_hbm,
    value_hbm,
    gated_hbm,
    layer_hbm,
    factor_value_hbm,
    factor_output_hbm,
    weight_value_hbm,
    weight_output_hbm,
    first_value_hbm,
    second_value_hbm,
    first_output_hbm,
    second_output_hbm,
    moments,
    step_value,
    step_output,
    next_value,
    next_output,
    final_value,
    final_output,
    directions,
    turned,
    factors,
    wide_value,
    wide_output,
    stream,
    cotan,
    weight_value,
    weight_output,
    old,
    flipped,
    out_x,
    in_x,
    out_z,
    in_z,
    totals,
    update_value,
    update_output,
    load_sem,
    send_sem,
    factor_recv,
    weight_recv,
    direction_recv,
    pair_recv,
    x_recv,
    z_recv,
    total_recv,
):
    fs, tp = lax.axis_index("fs"), lax.axis_index("tp")
    width = tp_size
    chips = fs_size // CORES
    depth = chips // width
    core, chip = lax.rem(fs, CORES), fs // CORES
    x, z = lax.rem(chip, width), chip // width
    rows, rank = factor_value_hbm.shape
    tokens = input_hbm.shape[0]
    cols = value_hbm.shape[1]
    ranks = first_value_hbm.shape[0]
    model = rows * fs_size
    last = depth - 1
    span = CORES * rows

    def index(z_at, x_at, core_at):
        return (z_at * width + x_at) * CORES + core_at

    def along_z(z_at):
        return {"fs": index(z_at, x, core)}

    over_x = {"fs": index(z, 1 - x, core)}
    over_core = {"fs": index(z, x, 1 - core)}
    over_y = {"tp": 1 - tp}
    beside = z + 1 - 2 * lax.rem(z, 2)
    mirror = last - z
    across = lax.rem(z + depth // 2, depth)
    others = (beside, mirror, across)
    middle = jnp.logical_and(z > 0, z < last)

    def block(ref, origin, size):
        return ref.at[pl.ds(pl.multiple_of(origin * size, size), size)]

    sources = (
        factor_value_hbm,
        factor_output_hbm,
        weight_value_hbm,
        weight_output_hbm,
        input_hbm,
        layer_hbm,
        value_hbm,
        gated_hbm,
        first_value_hbm,
        second_value_hbm,
        first_output_hbm,
        second_output_hbm,
    )
    targets = (
        block(factors.at[0], fs, rows),
        block(factors.at[1], fs, rows),
        weight_value,
        weight_output,
        stream.at[0],
        stream.at[1],
        cotan.at[0],
        cotan.at[1],
        old.at[0],
        old.at[1],
        old.at[2],
        old.at[3],
    )
    loads = [
        pltpu.make_async_copy(source, target, load_sem.at[slot])
        for slot, (source, target) in enumerate(zip(sources, targets))
    ]
    for load in loads:
        load.start()

    barrier = pltpu.get_barrier_semaphore()
    peers = [along_z(z_at) for z_at in others] + [over_x, over_core, over_y]
    for peer in peers:
        pl.semaphore_signal(barrier, inc=1, device_id=peer, device_id_type=MESH)
    loads[0].wait()
    loads[1].wait()
    pl.semaphore_wait(barrier, len(peers))

    sender = Sender(send_sem)

    def projected(kind):
        return (pl.ds(0, tokens), pl.ds(pl.multiple_of(kind * rank, rank), rank))

    def term_at(to, core_at):
        start = pl.multiple_of(tokens + (to * CORES + core_at) * ranks, ranks)
        return update_output.at[pl.ds(start, ranks), pl.ds(0, 2 * cols)]

    def paired_at(to):
        start = pl.multiple_of(tokens + rank + to * ranks, ranks)
        return update_output.at[pl.ds(start, ranks), pl.ds(0, 2 * cols)]

    def arrived(ref, recv_sem):
        pltpu.make_async_remote_copy(
            src_ref=ref,
            dst_ref=ref,
            send_sem=send_sem.at[0],
            recv_sem=recv_sem,
            device_id=over_core,
            device_id_type=MESH,
        ).wait_recv()

    def forward(ref, recv_sem, device, when=None):
        sender.send(ref, ref, recv_sem, device, when)

    mine, theirs = tp, 1 - tp

    def factor(kind, origin):
        return block(factors.at[kind], origin, rows), factor_recv.at[kind, origin]

    for z_at in others:
        forward(*factor(mine, fs), along_z(z_at))
    forward(*factor(mine, fs), over_x)
    forward(*factor(theirs, fs), over_x)
    forward(*factor(mine, fs), over_core)
    forward(*factor(theirs, fs), over_core)

    direct = (1,)
    lead, half_cols = rows // 2, cols // 2

    def piece(part, origin):
        start = pl.multiple_of(origin * rows, rows)
        if part < 2:
            ref = wide_value.at[pl.ds(start + part * lead, rows - lead if part else lead)]
        else:
            ref = wide_output.at[pl.ds((part - 2) * half_cols, half_cols), pl.ds(start, rows)]
        return ref, weight_recv.at[part, origin]

    def piece_z(part, origin):
        forward(*piece(part, origin), along_z(beside))
        forward(*piece(part, origin), along_z(mirror), middle)
        if part in direct:
            forward(*piece(part, origin), along_z(across))

    def piece_from_z(part, z_at, x_at, onward, when=None):
        ref, sem = piece(part, index(z_at, x_at, core))
        sender.guarded(lambda: arrived(ref, sem), when)
        if onward is not None:
            forward(ref, sem, along_z(onward), middle)
        forward(ref, sem, over_core, when)

    def near(part, x_at):
        relayed = part not in direct
        piece_from_z(part, beside, x_at, mirror if relayed else None)
        piece_from_z(part, mirror, x_at, beside if relayed else None, middle)

    def second(part, x_at):
        piece_from_z(part, across, x_at, beside)

    def third(part, x_at):
        piece_from_z(part, mirror, x_at, None, jnp.logical_not(middle))

    def cross(part, *z_ats):
        for z_at in z_ats:
            forward(*piece(part, index(z_at, x, core)), over_x)

    def to_core(part, *z_ats):
        for z_at in z_ats:
            forward(*piece(part, index(z_at, x, core)), over_core)

    def from_x(part, *z_ats):
        for z_at in z_ats:
            ref, sem = piece(part, index(z_at, 1 - x, core))
            arrived(ref, sem)
            forward(ref, sem, over_core)

    loads[2].wait()
    loads[3].wait()
    own_rows = pl.ds(pl.multiple_of(fs * rows, rows), rows)
    wide_value[own_rows, :] = weight_value[...].astype(jnp.bfloat16)
    wide_output[:, own_rows] = weight_output[...].astype(jnp.bfloat16)
    cross(0, z)
    piece_z(1, fs)
    piece_z(2, fs)
    piece_z(3, fs)

    for z_at in others:
        ref, sem = factor(mine, index(z_at, x, core))
        arrived(ref, sem)
        forward(ref, sem, over_x)
        forward(ref, sem, over_y)
        forward(ref, sem, over_core)
    for part in (1, 2, 3):
        cross(part, z)
    ref, sem = factor(theirs, index(z, 1 - x, core))
    arrived(ref, sem)
    forward(ref, sem, over_core)
    for z_at in (z,) + others:
        ref, sem = factor(mine, index(z_at, 1 - x, core))
        arrived(ref, sem)
        if z_at is not z:
            forward(ref, sem, over_y)
        forward(ref, sem, over_core)
    for load in loads[4:]:
        load.wait()

    def project(kind, z_at, x_at, first=False):
        arrived(*factor(kind, index(z_at, x_at, 1 - core)))
        part = pl.ds(pl.multiple_of((z_at * width + x_at) * span, span), span)
        product = jnp.dot(
            stream[kind, :, part], factors[kind, part], preferred_element_type=jnp.float32
        )
        at = projected(kind)
        update_output[at] = product if first else update_output[at] + product

    def from_y(z_at, x_at):
        ref, sem = factor(theirs, index(z_at, x_at, core))
        arrived(ref, sem)
        forward(ref, sem, over_core)

    project(mine, z, x, True)
    project(theirs, z, x, True)
    for z_at in others:
        project(mine, z_at, x)
    for z_at in others:
        from_y(z_at, x)
    for z_at in (z,) + others:
        project(mine, z_at, 1 - x)
    for z_at in others:
        from_y(z_at, 1 - x)
    for part in range(4):
        to_core(part, z)
    near(1, x)
    for z_at in others:
        project(theirs, z_at, x)
    for z_at in (z,) + others:
        project(theirs, z_at, 1 - x)

    second(1, x)
    near(2, x)
    cross(1, beside)
    width_tile = 256
    for kind in range(2):
        flipped[...] = update_output[projected(kind)].T.astype(jnp.bfloat16)

        @pl.loop(0, cols // width_tile)
        def _(step, kind=kind):
            tile = pl.ds(pl.multiple_of(step * width_tile, width_tile), width_tile)
            term = jnp.dot(flipped[...], cotan[kind, :, tile], preferred_element_type=jnp.float32)
            target = pl.ds(pl.multiple_of(kind * cols + step * width_tile, width_tile), width_tile)
            update_output[tokens : tokens + rank, target] = term

    far = others + (z,)
    for x_at in (1 - x, x):
        for z_at in far:
            to = z_at * width + x_at
            sender.send(term_at(to, 1 - core), paired_at(to), pair_recv.at[to], over_core)

    def pair_sum(z_at, x_at):
        at = z_at * width + x_at
        arrived(paired_at(at), pair_recv.at[at])
        return term_at(at, core)[...] + paired_at(at)[...]

    for z_at in far:
        out_x[z_at] = pair_sum(z_at, 1 - x).astype(jnp.bfloat16)
        sender.send(out_x.at[z_at], in_x.at[z_at], x_recv.at[z_at], over_x)
    cross(1, across)
    near(3, x)
    from_x(0, z)

    def column_sum(z_at):
        total = pair_sum(z_at, x)
        arrived(in_x.at[z_at], x_recv.at[z_at])
        return total + in_x[z_at].astype(jnp.float32)

    for z_at in others:
        out_z[z_at] = column_sum(z_at).astype(jnp.bfloat16)
        sender.send(out_z.at[z_at], in_z.at[z], z_recv.at[z], along_z(z_at))
    early = len(sender.pending)
    low = column_sum(z)
    second(2, x)
    piece_z(0, fs)
    for part in (1, 2, 3):
        from_x(part, z)
    for z_at in others:
        arrived(in_z.at[z_at], z_recv.at[z_at])
        low = low + in_z[z_at].astype(jnp.float32)

    own_ranks = pl.ds(pl.multiple_of(fs * ranks, ranks), ranks)
    for kind in range(2):
        part = low[:, kind * cols : (kind + 1) * cols]
        next_first, next_second = next_moments(old[2 * kind], old[2 * kind + 1], part)
        moments[2 * kind] = next_first
        moments[2 * kind + 1] = next_second
        directions[own_ranks, kind * cols : (kind + 1) * cols] = (
            next_first * lax.rsqrt(next_second)
        ).astype(jnp.bfloat16)

    def direction(origin):
        return block(directions, origin, ranks), direction_recv.at[origin]

    for z_at in others:
        forward(*direction(fs), along_z(z_at))
    forward(*direction(fs), over_x)
    forward(*direction(fs), over_core)
    cross(2, beside)
    second(3, x)
    cross(3, beside)
    piece_z(0, index(z, 1 - x, core))
    for z_at in others:
        ref, sem = direction(index(z_at, x, core))
        arrived(ref, sem)
        forward(ref, sem, over_x)
        forward(ref, sem, over_core)
    cross(2, across)
    third(1, x)
    cross(1, mirror)
    near(0, x)
    from_x(1, beside, across)
    for z_at in (z,) + others:
        ref, sem = direction(index(z_at, 1 - x, core))
        arrived(ref, sem)
        forward(ref, sem, over_core)
    for z_at in (z,) + others:
        for x_at in (x, 1 - x):
            arrived(*direction(index(z_at, x_at, 1 - core)))
    def total_of(kind):
        totals[tp, kind] = jnp.zeros((8, cols), jnp.float32)

        @pl.loop(0, chips)
        def _(step):
            part = pl.ds(pl.multiple_of(step * span, span), span)
            if kind == 0:
                update = jnp.dot(
                    factors[0, part], directions[:, :cols], preferred_element_type=jnp.float32
                )
                update_value[part] = update
            else:
                update = lax.dot_general(
                    turned[...],
                    factors[1, part],
                    (((1,), (1,)), ((), ())),
                    preferred_element_type=jnp.float32,
                )
                update_output[:, part] = update
            square = update * update
            lanes = square.shape[1]
            totals[tp, kind, :, :lanes] += jnp.sum(square.reshape(-1, 8, lanes), axis=0)

    cross(3, across)
    third(2, x)
    cross(2, mirror)
    near(0, 1 - x)
    sender.drain(early)
    total_of(0)
    second(0, x)
    third(3, x)
    cross(3, mirror)
    turned[...] = directions[:, cols:].astype(jnp.float32).T.astype(jnp.bfloat16)
    total_of(1)
    sender.send(totals.at[tp], totals.at[tp], total_recv.at[tp], over_y)
    second(0, 1 - x)
    from_x(1, mirror)
    from_x(2, beside, across)
    from_x(3, beside)
    arrived(totals.at[1 - tp], total_recv.at[1 - tp])
    entries = model * cols * tp_size
    scales = [
        lax.rsqrt(jnp.sum(totals[0, kind] + totals[1, kind], keepdims=True) / entries + 1e-06)
        for kind in range(2)
    ]
    def finals(kind, z_at, x_at):
        for part in (2 * kind, 2 * kind + 1):
            arrived(*piece(part, index(z_at, x_at, 1 - core)))
        part = pl.ds(pl.multiple_of((z_at * width + x_at) * span, span), span)
        scale = 0.02 * scales[kind]
        if kind == 0:
            final_value[part] = (
                wide_value[part].astype(jnp.float32) - update_value[part] * scale
            ).astype(jnp.bfloat16)
        else:
            final_output[:, part] = (
                wide_output[:, part].astype(jnp.float32) - update_output[:, part] * scale
            ).astype(jnp.bfloat16)

    step = update_value[own_rows] * scales[0]
    step_value[...] = step
    next_value[...] = weight_value[...] - 0.02 * step
    step = update_output[:, own_rows] * scales[1]
    step_output[...] = step
    next_output[...] = weight_output[...] - 0.02 * step
    finals(0, z, x)
    finals(1, z, x)
    finals(1, beside, x)
    from_x(3, across)
    third(0, x)
    finals(0, beside, x)
    finals(0, across, x)
    finals(1, across, x)
    from_x(2, mirror)
    finals(1, z, 1 - x)
    third(0, 1 - x)
    for z_at in (z, beside, across):
        finals(0, z_at, 1 - x)
    finals(1, beside, 1 - x)
    from_x(3, mirror)
    finals(0, mirror, x)
    finals(1, mirror, x)
    finals(0, mirror, 1 - x)
    finals(1, across, 1 - x)
    finals(1, mirror, 1 - x)
    sender.drain()


def write(count, *refs):
    sems = refs[-1]
    copies = [
        pltpu.make_async_copy(source, target, sems.at[slot])
        for slot, (source, target) in enumerate(
            zip(refs[1:count] + tuple(refs[0].at[k] for k in range(4)), refs[count:-1])
        )
    ]
    for copy in copies:
        copy.start()
    for copy in copies:
        copy.wait()


def fused_body(fs_size, tp_size, *args):
    tokens, model = args[0].shape
    cols = args[1].shape[1]
    rows, rank = args[4].shape
    ranks = args[8].shape[0]
    chips = fs_size // CORES
    depth = chips // tp_size
    f32, bf16 = jnp.float32, jnp.bfloat16
    vmem = pl.BlockSpec(memory_space=pltpu.VMEM)
    hbm = pl.BlockSpec(memory_space=pltpu.HBM)
    shape = jax.ShapeDtypeStruct
    dma = pltpu.SemaphoreType.DMA
    args = [pltpu.with_memory_space_constraint(arg, pltpu.HBM) for arg in args]
    own = [shape((rows, cols), f32), shape((cols, rows), f32)] * 2
    copies = [shape((model, cols), bf16), shape((cols, model), bf16)]
    results = pl.pallas_call(
        functools.partial(fused, fs_size, tp_size),
        out_shape=[shape((4, ranks, cols), f32)] + own + copies,
        in_specs=[hbm] * 12,
        out_specs=[vmem] * 7,
        scratch_shapes=[
            pltpu.VMEM((rank, 2 * cols), bf16),
            pltpu.VMEM((cols, rank), bf16),
            pltpu.VMEM((2, model, rank), bf16),
            pltpu.VMEM((model, cols), bf16),
            pltpu.VMEM((cols, model), bf16),
            pltpu.VMEM((2, tokens, model), bf16),
            pltpu.VMEM((2, tokens, cols), bf16),
            pltpu.VMEM((rows, cols), f32),
            pltpu.VMEM((cols, rows), f32),
            pltpu.VMEM((4, ranks, cols), f32),
            pltpu.VMEM((rank, tokens), bf16),
        ]
        + [pltpu.VMEM((depth, ranks, 2 * cols), bf16)] * 4
        + [
            pltpu.VMEM((tp_size, 2, 8, cols), f32),
            pltpu.VMEM((model, cols), f32),
            pltpu.VMEM((cols, model), f32),
            dma((12,)),
            dma((136,)),
            dma((2, fs_size)),
            dma((4, fs_size)),
            dma((fs_size,)),
            dma((chips,)),
            dma((depth,)),
            dma((depth,)),
            dma((tp_size,)),
        ],
        compiler_params=pltpu.CompilerParams(
            collective_id=0, has_side_effects=True, vmem_limit_bytes=40 * 1024 * 1024
        ),
    )(*args)

    written = pl.pallas_call(
        functools.partial(write, len(results)),
        out_shape=own + copies + [shape((ranks, cols), f32)] * 4,
        in_specs=[vmem] * len(results),
        out_specs=[hbm] * 10,
        scratch_shapes=[dma((10,))],
        compiler_params=pltpu.CompilerParams(vmem_limit_bytes=1024 * 1024),
    )(*results)
    return written[:4] + written[6:] + written[4:6]


def solution(mesh):
    fs_size, tp_size = mesh.shape["fs"], mesh.shape["tp"]
    placed = (
        P("fs", None),
        P("fs", "tp"),
        P("fs", "tp"),
        P("fs", None),
        P("fs", None),
        P("fs", None),
        P("fs", "tp"),
        P("tp", "fs"),
        P("fs", "tp"),
        P("fs", "tp"),
        P("fs", "tp"),
        P("fs", "tp"),
    )
    chips = fs_size // CORES
    tiled = tp_size == 2 and fs_size == 16 and chips % tp_size == 0
    return jax.shard_map(
        functools.partial(fused_body, fs_size, tp_size) if tiled else body,
        mesh=mesh,
        in_specs=placed,
        out_specs=(
            P("fs", "tp"),
            P("tp", "fs"),
            P("fs", "tp"),
            P("tp", "fs"),
            P("fs", "tp"),
            P("fs", "tp"),
            P("fs", "tp"),
            P("fs", "tp"),
            P(None, "tp"),
            P("tp", None),
        ),
        check_vma=False,
    )
```

```python
import functools

import jax
import jax.numpy as jnp
from jax import lax
from jax.experimental import pallas as pl
from jax.experimental.pallas import tpu as pltpu
from jax.sharding import PartitionSpec as P

CORES = 2

D = 2048
WIDTH = 2048


def gram_times(gram_matrix, directions):
    gram_high = gram_matrix.astype(jnp.bfloat16)
    gram_low = (gram_matrix - gram_high.astype(jnp.float32)).astype(jnp.bfloat16)
    return jnp.dot(gram_high, directions, preferred_element_type=jnp.float32) + jnp.dot(
        gram_low, directions, preferred_element_type=jnp.float32
    )


def body(
    normed_input,
    value_cotangent,
    gated_output,
    layer_cotangent,
    factor_value,
    factor_output,
    weight_value,
    weight_output,
    first_value,
    second_value,
    first_output,
    second_output,
):
    col_count = value_cotangent.shape[1]
    inner = (((0,), (0,)), ((), ()))
    pieces = (
        lax.all_gather(factor_value, "fs", axis=0, tiled=True),
        lax.all_gather(factor_output, "fs", axis=0, tiled=True),
    )
    piece_value, piece_output = pieces
    span_input = normed_input
    span_cotan = layer_cotangent
    gram_value = lax.dot_general(pieces[0], pieces[0], inner, preferred_element_type=jnp.float32)
    gram_output = lax.dot_general(pieces[1], pieces[1], inner, preferred_element_type=jnp.float32)
    projected_input = jnp.dot(span_input, piece_value, preferred_element_type=jnp.float32).astype(
        jnp.bfloat16
    )
    projected_cotangent = jnp.dot(
        span_cotan, piece_output, preferred_element_type=jnp.float32
    ).astype(jnp.bfloat16)
    span_input = projected_input
    span_cotan = projected_cotangent
    term_value = lax.dot_general(
        span_input, value_cotangent, inner, preferred_element_type=jnp.float32
    )
    term_output = lax.dot_general(
        span_cotan, gated_output, inner, preferred_element_type=jnp.float32
    )
    low_rank = lax.psum_scatter(
        jnp.concatenate([term_value, term_output], axis=1), "fs", scatter_dimension=0, tiled=True
    )
    low_value = low_rank[:, :col_count]
    low_output = low_rank[:, col_count:]
    next_first_value = 0.9 * first_value + 0.1 * low_value
    next_second_value = 0.95 * second_value + 0.05 * low_value * low_value
    next_first_output = 0.9 * first_output + 0.1 * low_output
    next_second_output = 0.95 * second_output + 0.05 * low_output * low_output
    direction_value = (next_first_value * lax.rsqrt(next_second_value)).astype(jnp.bfloat16)
    direction_output = (next_first_output * lax.rsqrt(next_second_output)).astype(jnp.bfloat16)
    gathered_value, gathered_output = (
        lax.all_gather(direction_value, "fs", axis=0, tiled=True),
        lax.all_gather(direction_output, "fs", axis=0, tiled=True),
    )
    update_value = jnp.dot(factor_value, gathered_value, preferred_element_type=jnp.float32)
    update_output = lax.dot_general(
        gathered_output, factor_output, (((0,), (1,)), ((), ())), preferred_element_type=jnp.float32
    )
    square_value = jnp.sum(
        gathered_value.astype(jnp.float32) * gram_times(gram_value, gathered_value)
    )
    square_output = jnp.sum(
        gathered_output.astype(jnp.float32) * gram_times(gram_output, gathered_output)
    )
    total_value, total_output = lax.psum((square_value, square_output), "tp")
    entries = D * WIDTH
    step_value = update_value * lax.rsqrt(total_value / entries + 1e-06)
    step_output = update_output * lax.rsqrt(total_output / entries + 1e-06)
    next_weight_value = weight_value - 0.02 * step_value
    next_weight_output = weight_output - 0.02 * step_output
    half_value = next_weight_value.astype(jnp.bfloat16)
    half_output = next_weight_output.astype(jnp.bfloat16)
    copy_value, copy_output = (
        lax.all_gather(half_value, "fs", axis=0, tiled=True),
        lax.all_gather(half_output, "fs", axis=1, tiled=True),
    )
    return (
        step_value,
        step_output,
        next_weight_value,
        next_weight_output,
        next_first_value,
        next_second_value,
        next_first_output,
        next_second_output,
        copy_value,
        copy_output,
    )


def next_moments(first, second, low):
    return 0.9 * first + 0.1 * low, 0.95 * second + 0.05 * low * low


MESH = pl.DeviceIdType.MESH


class Sender:
    def __init__(self, sems):
        self.sems, self.pending, self.drained = sems, [], 0

    def send(self, source, target, recv_sem, device, when=None):
        slots = self.sems.shape[0]
        self.drain(len(self.pending) + 1 - slots)
        copy = pltpu.make_async_remote_copy(
            src_ref=source,
            dst_ref=target,
            send_sem=self.sems.at[len(self.pending) % slots],
            recv_sem=recv_sem,
            device_id=device,
            device_id_type=MESH,
        )
        self.guarded(copy.start, when)
        self.pending.append((copy, when))

    def guarded(self, action, when):
        if when is None:
            action()
        else:

            @pl.when(when)
            def _():
                action()

    def drain(self, count=None):
        count = max(len(self.pending) if count is None else count, self.drained)
        for copy, when in self.pending[self.drained : count]:
            self.guarded(copy.wait_send, when)
        self.drained = count


def fused(
    fs_size,
    tp_size,
    input_hbm,
    value_hbm,
    gated_hbm,
    layer_hbm,
    factor_value_hbm,
    factor_output_hbm,
    weight_value_hbm,
    weight_output_hbm,
    first_value_hbm,
    second_value_hbm,
    first_output_hbm,
    second_output_hbm,
    moments,
    step_value,
    step_output,
    next_value,
    next_output,
    final_value,
    final_output,
    directions,
    turned,
    factors,
    wide_value,
    wide_output,
    stream,
    cotan,
    weight_value,
    weight_output,
    old,
    flipped,
    out_x,
    in_x,
    out_z,
    in_z,
    squares,
    totals,
    update_value,
    update_output,
    load_sem,
    send_sem,
    factor_recv,
    weight_recv,
    core_recv,
    direction_recv,
    join_recv,
    pair_recv,
    x_recv,
    z_recv,
    total_recv,
):
    fs, tp = lax.axis_index("fs"), lax.axis_index("tp")
    width = tp_size
    chips = fs_size // CORES
    depth = chips // width
    core, chip = lax.rem(fs, CORES), fs // CORES
    x, z = lax.rem(chip, width), chip // width
    rows, rank = factor_value_hbm.shape
    tokens = input_hbm.shape[0]
    cols = value_hbm.shape[1]
    ranks = first_value_hbm.shape[0]
    model = rows * fs_size
    last = depth - 1
    span = CORES * rows

    def index(z_at, x_at, core_at):
        return (z_at * width + x_at) * CORES + core_at

    def along_z(z_at):
        return {"fs": index(z_at, x, core)}

    over_x = {"fs": index(z, 1 - x, core)}
    over_core = {"fs": index(z, x, 1 - core)}
    over_y = {"tp": 1 - tp}
    diagonal = {**over_core, **over_y}
    beside = z + 1 - 2 * lax.rem(z, 2)
    mirror = last - z
    across = lax.rem(z + depth // 2, depth)
    others = (beside, mirror, across)
    middle = jnp.logical_and(z > 0, z < last)

    barrier = pltpu.get_barrier_semaphore()
    peers = [along_z(z_at) for z_at in others] + [over_x, over_core, over_y, diagonal]
    for peer in peers:
        pl.semaphore_signal(barrier, inc=1, device_id=peer, device_id_type=MESH)
    def block(ref, origin, size):
        return ref.at[pl.ds(pl.multiple_of(origin * size, size), size)]

    sources = (
        factor_value_hbm,
        factor_output_hbm,
        weight_value_hbm,
        weight_output_hbm,
        input_hbm,
        layer_hbm,
        value_hbm,
        gated_hbm,
        first_value_hbm,
        second_value_hbm,
        first_output_hbm,
        second_output_hbm,
    )
    targets = (
        block(factors.at[0], fs, rows),
        block(factors.at[1], fs, rows),
        weight_value,
        weight_output,
        stream.at[0],
        stream.at[1],
        cotan.at[0],
        cotan.at[1],
        old.at[0],
        old.at[1],
        old.at[2],
        old.at[3],
    )
    loads = [
        pltpu.make_async_copy(source, target, load_sem.at[slot])
        for slot, (source, target) in enumerate(zip(sources, targets))
    ]
    for load in loads:
        load.start()

    loads[0].wait()
    loads[1].wait()
    pl.semaphore_wait(barrier, len(peers))

    sender = Sender(send_sem)

    def projected(kind):
        return (pl.ds(0, tokens), pl.ds(pl.multiple_of(kind * rank, rank), rank))

    def term_at(to, core_at):
        start = pl.multiple_of(tokens + (to * CORES + core_at) * ranks, ranks)
        return update_output.at[pl.ds(start, ranks), pl.ds(0, 2 * cols)]

    def paired_at(to):
        start = pl.multiple_of(tokens + rank + to * ranks, ranks)
        return update_output.at[pl.ds(start, ranks), pl.ds(0, 2 * cols)]

    def arrived(ref, recv_sem):
        pltpu.make_async_remote_copy(
            src_ref=ref,
            dst_ref=ref,
            send_sem=send_sem.at[0],
            recv_sem=recv_sem,
            device_id=over_core,
            device_id_type=MESH,
        ).wait_recv()

    def forward(ref, recv_sem, device, when=None):
        sender.send(ref, ref, recv_sem, device, when)

    mine, theirs = tp, 1 - tp

    def factor(kind, origin):
        return block(factors.at[kind], origin, rows), factor_recv.at[kind, origin]

    for z_at in others:
        forward(*factor(mine, fs), along_z(z_at))
    forward(*factor(mine, fs), over_x)
    forward(*factor(theirs, fs), over_x)
    forward(*factor(mine, fs), over_core)
    forward(*factor(theirs, fs), over_core)

    direct = (1,)
    lead, half_cols = rows * 3 // 8, cols // 2

    def piece(part, origin):
        start = pl.multiple_of(origin * rows, rows)
        if part < 2:
            ref = wide_value.at[pl.ds(start + part * lead, rows - lead if part else lead)]
        else:
            ref = wide_output.at[pl.ds((part - 2) * half_cols, half_cols), pl.ds(start, rows)]
        return ref, weight_recv.at[part, origin // CORES]

    def piece_to_core(part, origin, when=None):
        ref, _ = piece(part, origin)
        forward(ref, core_recv.at[part // 2, origin // CORES], over_core, when)

    def piece_z(part, origin):
        forward(*piece(part, origin), along_z(beside))
        forward(*piece(part, origin), along_z(mirror), middle)
        if part in direct:
            forward(*piece(part, origin), along_z(across))

    def piece_from_z(part, z_at, x_at, onward, when=None):
        ref, sem = piece(part, index(z_at, x_at, core))
        sender.guarded(lambda: arrived(ref, sem), when)
        if onward is not None:
            forward(ref, sem, along_z(onward), middle)
        piece_to_core(part, index(z_at, x_at, core), when)

    def near(part, x_at):
        relayed = part not in direct
        piece_from_z(part, beside, x_at, mirror if relayed else None)
        piece_from_z(part, mirror, x_at, beside if relayed else None, middle)

    def second(part, x_at):
        piece_from_z(part, across, x_at, beside)

    def third(part, x_at):
        piece_from_z(part, mirror, x_at, None, jnp.logical_not(middle))

    def cross(part, *z_ats):
        for z_at in z_ats:
            forward(*piece(part, index(z_at, x, core)), over_x)

    def to_core(part, *z_ats):
        for z_at in z_ats:
            piece_to_core(part, index(z_at, x, core))

    def from_x(part, *z_ats):
        for z_at in z_ats:
            arrived(*piece(part, index(z_at, 1 - x, core)))
            piece_to_core(part, index(z_at, 1 - x, core))

    loads[2].wait()
    loads[3].wait()
    own_rows = pl.ds(pl.multiple_of(fs * rows, rows), rows)
    wide_value[own_rows, :] = weight_value[...].astype(jnp.bfloat16)
    wide_output[:, own_rows] = weight_output[...].astype(jnp.bfloat16)
    cross(0, z)
    piece_z(1, fs)
    piece_z(2, fs)
    piece_z(3, fs)

    for z_at in others:
        ref, sem = factor(mine, index(z_at, x, core))
        arrived(ref, sem)
        forward(ref, sem, over_x)
        forward(ref, sem, over_y)
        forward(ref, sem, over_core)
    for part in (1, 2, 3):
        cross(part, z)
    ref, sem = factor(theirs, index(z, 1 - x, core))
    arrived(ref, sem)
    forward(ref, sem, over_core)
    for z_at in (z,) + others:
        ref, sem = factor(mine, index(z_at, 1 - x, core))
        arrived(ref, sem)
        if z_at is not z:
            forward(ref, sem, over_y)
        forward(ref, sem, over_core)
    for load in loads[4:]:
        load.wait()

    def project(kind, z_at, x_at, first=False):
        arrived(*factor(kind, index(z_at, x_at, 1 - core)))
        part = pl.ds(pl.multiple_of((z_at * width + x_at) * span, span), span)
        product = jnp.dot(
            stream[kind, :, part], factors[kind, part], preferred_element_type=jnp.float32
        )
        at = projected(kind)
        update_output[at] = product if first else update_output[at] + product

    def from_y(z_at, x_at):
        ref, sem = factor(theirs, index(z_at, x_at, core))
        arrived(ref, sem)
        forward(ref, sem, over_core)

    project(mine, z, x, True)
    project(theirs, z, x, True)
    for z_at in others:
        project(mine, z_at, x)
    for z_at in others:
        from_y(z_at, x)
    for z_at in (z,) + others:
        project(mine, z_at, 1 - x)
    for z_at in others:
        from_y(z_at, 1 - x)
    for part in range(4):
        to_core(part, z)
    near(1, x)
    for z_at in others:
        project(theirs, z_at, x)
    for z_at in (z,) + others:
        project(theirs, z_at, 1 - x)

    second(1, x)
    cross(1, beside)
    width_tile = 256
    for kind in range(2):
        flipped[...] = update_output[projected(kind)].T.astype(jnp.bfloat16)

        @pl.loop(0, cols // width_tile)
        def _(step, kind=kind):
            tile = pl.ds(pl.multiple_of(step * width_tile, width_tile), width_tile)
            term = jnp.dot(flipped[...], cotan[kind, :, tile], preferred_element_type=jnp.float32)
            target = pl.ds(pl.multiple_of(kind * cols + step * width_tile, width_tile), width_tile)
            update_output[tokens : tokens + rank, target] = term

    far = others + (z,)
    for x_at in (1 - x, x):
        for z_at in far:
            to = z_at * width + x_at
            sender.send(term_at(to, 1 - core), paired_at(to), pair_recv.at[to], over_core)

    def pair_sum(z_at, x_at):
        at = z_at * width + x_at
        arrived(paired_at(at), pair_recv.at[at])
        return term_at(at, core)[...] + paired_at(at)[...]

    for z_at in far:
        out_x[z_at] = pair_sum(z_at, 1 - x).astype(jnp.bfloat16)
        sender.send(out_x.at[z_at], in_x.at[z_at], x_recv.at[z_at], over_x)
    near(2, x)
    cross(1, across)
    near(3, x)
    from_x(0, z)

    def column_sum(z_at):
        total = pair_sum(z_at, x)
        arrived(in_x.at[z_at], x_recv.at[z_at])
        return total + in_x[z_at].astype(jnp.float32)

    for z_at in others:
        out_z[z_at] = column_sum(z_at).astype(jnp.bfloat16)
        sender.send(out_z.at[z_at], in_z.at[z], z_recv.at[z], along_z(z_at))
    early = len(sender.pending)
    low = column_sum(z)
    cross(2, beside)
    second(2, x)
    for part in (1, 2, 3):
        from_x(part, z)
    for z_at in others:
        arrived(in_z.at[z_at], z_recv.at[z_at])
        low = low + in_z[z_at].astype(jnp.float32)

    own_ranks = pl.ds(pl.multiple_of(fs * ranks, ranks), ranks)
    for kind in range(2):
        part = low[:, kind * cols : (kind + 1) * cols]
        next_first, next_second = next_moments(old[2 * kind], old[2 * kind + 1], part)
        moments[2 * kind] = next_first
        moments[2 * kind + 1] = next_second
        directions[own_ranks, kind * cols : (kind + 1) * cols] = (
            next_first * lax.rsqrt(next_second)
        ).astype(jnp.bfloat16)

    def direction(origin):
        return block(directions, origin, ranks), direction_recv.at[origin // CORES]

    for z_at in others:
        forward(*direction(fs), along_z(z_at))
    forward(*direction(fs), over_x)
    forward(direction(fs)[0], join_recv.at[0], over_core)
    cross(3, beside)
    cross(2, across)
    piece_z(0, fs)
    second(3, x)
    piece_z(0, index(z, 1 - x, core))
    for z_at in others:
        ref, sem = direction(index(z_at, x, core))
        arrived(ref, sem)
        forward(ref, sem, over_x)
        forward(ref, join_recv.at[0], over_core)
    third(1, x)
    cross(1, mirror)
    from_x(1, beside, across)
    for z_at in (z,) + others:
        ref, sem = direction(index(z_at, 1 - x, core))
        arrived(ref, sem)
        forward(ref, join_recv.at[0], over_core)
    near(0, x)
    cross(3, across)
    third(2, x)
    cross(2, mirror)
    arrived(directions.at[pl.ds(0, chips * ranks)], join_recv.at[0])
    half = chips // CORES
    me = tp * CORES + core

    def updates(kind, side, counted):
        if counted:
            squares[kind] = jnp.zeros((8, cols), jnp.float32)

        @pl.loop(0, half)
        def _(step):
            part = pl.ds(pl.multiple_of((side * half + step) * span, span), span)
            if kind == 0:
                update = jnp.dot(
                    factors[0, part], directions[:, :cols], preferred_element_type=jnp.float32
                )
                update_value[part] = update
            else:
                update = lax.dot_general(
                    turned[...],
                    factors[1, part],
                    (((1,), (1,)), ((), ())),
                    preferred_element_type=jnp.float32,
                )
                update_output[:, part] = update
            if counted:
                square = update * update
                lanes = square.shape[1]
                squares[kind, :, :lanes] += jnp.sum(square.reshape(-1, 8, lanes), axis=0)

        if counted:
            folded = squares[kind, :, :128]
            for lane in range(128, cols, 128):
                folded = folded + squares[kind, :, lane : lane + 128]
            totals[me, kind] = folded

    sender.drain(early)
    updates(0, core, True)
    near(0, 1 - x)
    turned[...] = directions[:, cols:].astype(jnp.float32).T.astype(jnp.bfloat16)
    second(0, x)
    third(3, x)
    cross(3, mirror)
    updates(1, core, True)
    for device in (over_y, over_core, diagonal):
        sender.send(totals.at[me], totals.at[me], total_recv.at[me], device)
    second(0, 1 - x)
    updates(0, 1 - core, False)
    updates(1, 1 - core, False)
    from_x(1, mirror)
    from_x(2, beside, across)
    from_x(3, beside)
    for tp_at, core_at in ((tp, 1 - core), (1 - tp, core), (1 - tp, 1 - core)):
        slot = tp_at * CORES + core_at
        arrived(totals.at[slot], total_recv.at[slot])
    entries = model * cols * tp_size
    scales = [
        lax.rsqrt(jnp.sum(jnp.sum(totals[:, kind], axis=0), keepdims=True) / entries + 1e-06)
        for kind in range(2)
    ]
    def finals(kind, z_at, x_at):
        at = z_at * width + x_at
        sent = pl.ds(pl.multiple_of((at * CORES + 1 - core) * rows, rows), rows)
        arrived((wide_output.at[:, sent] if kind else wide_value.at[sent]), core_recv.at[kind, at])
        part = pl.ds(pl.multiple_of((z_at * width + x_at) * span, span), span)
        scale = 0.02 * scales[kind]
        if kind == 0:
            final_value[part] = (
                wide_value[part].astype(jnp.float32) - update_value[part] * scale
            ).astype(jnp.bfloat16)
        else:
            final_output[:, part] = (
                wide_output[:, part].astype(jnp.float32) - update_output[:, part] * scale
            ).astype(jnp.bfloat16)

    step = update_value[own_rows] * scales[0]
    step_value[...] = step
    next_value[...] = weight_value[...] - 0.02 * step
    step = update_output[:, own_rows] * scales[1]
    step_output[...] = step
    next_output[...] = weight_output[...] - 0.02 * step
    finals(0, z, x)
    finals(1, z, x)
    finals(1, beside, x)
    from_x(3, across)
    third(0, x)
    finals(0, beside, x)
    finals(0, across, x)
    finals(1, across, x)
    from_x(2, mirror)
    finals(1, z, 1 - x)
    third(0, 1 - x)
    for z_at in (z, beside, across):
        finals(0, z_at, 1 - x)
    finals(1, beside, 1 - x)
    from_x(3, mirror)
    finals(0, mirror, x)
    finals(1, mirror, x)
    finals(0, mirror, 1 - x)
    finals(1, across, 1 - x)
    finals(1, mirror, 1 - x)
    sender.drain()


def write(count, *refs):
    sems = refs[-1]
    sources = refs[5:count] + refs[1:5] + tuple(refs[0].at[k] for k in range(4))
    targets = refs[count + 4 : count + 6] + refs[count : count + 4] + refs[count + 6 : -1]
    copies = [
        pltpu.make_async_copy(source, target, sems.at[slot])
        for slot, (source, target) in enumerate(zip(sources, targets))
    ]
    for copy in copies:
        copy.start()
    for copy in copies:
        copy.wait()


def fused_body(fs_size, tp_size, *args):
    tokens, model = args[0].shape
    cols = args[1].shape[1]
    rows, rank = args[4].shape
    ranks = args[8].shape[0]
    chips = fs_size // CORES
    depth = chips // tp_size
    f32, bf16 = jnp.float32, jnp.bfloat16
    vmem = pl.BlockSpec(memory_space=pltpu.VMEM)
    hbm = pl.BlockSpec(memory_space=pltpu.HBM)
    shape = jax.ShapeDtypeStruct
    dma = pltpu.SemaphoreType.DMA
    args = [pltpu.with_memory_space_constraint(arg, pltpu.HBM) for arg in args]
    own = [shape((rows, cols), f32), shape((cols, rows), f32)] * 2
    copies = [shape((model, cols), bf16), shape((cols, model), bf16)]
    results = pl.pallas_call(
        functools.partial(fused, fs_size, tp_size),
        out_shape=[shape((4, ranks, cols), f32)] + own + copies,
        in_specs=[hbm] * 12,
        out_specs=[vmem] * 7,
        scratch_shapes=[
            pltpu.VMEM((rank, 2 * cols), bf16),
            pltpu.VMEM((cols, rank), bf16),
            pltpu.VMEM((2, model, rank), bf16),
            pltpu.VMEM((model, cols), bf16),
            pltpu.VMEM((cols, model), bf16),
            pltpu.VMEM((2, tokens, model), bf16),
            pltpu.VMEM((2, tokens, cols), bf16),
            pltpu.VMEM((rows, cols), f32),
            pltpu.VMEM((cols, rows), f32),
            pltpu.VMEM((4, ranks, cols), f32),
            pltpu.VMEM((rank, tokens), bf16),
        ]
        + [pltpu.VMEM((depth, ranks, 2 * cols), bf16)] * 4
        + [
            pltpu.VMEM((2, 8, cols), f32),
            pltpu.VMEM((tp_size * CORES, 2, 8, 128), f32),
            pltpu.VMEM((model, cols), f32),
            pltpu.VMEM((cols, model), f32),
            dma((12,)),
            dma((40,)),
            dma((2, fs_size)),
            dma((4, chips)),
            dma((2, chips)),
            dma((chips,)),
            dma((1,)),
            dma((chips,)),
            dma((depth,)),
            dma((depth,)),
            dma((tp_size * CORES,)),
        ],
        compiler_params=pltpu.CompilerParams(
            collective_id=0, has_side_effects=True, vmem_limit_bytes=40 * 1024 * 1024
        ),
    )(*args)

    written = pl.pallas_call(
        functools.partial(write, len(results)),
        out_shape=own + copies + [shape((ranks, cols), f32)] * 4,
        in_specs=[vmem] * len(results),
        out_specs=[hbm] * 10,
        scratch_shapes=[dma((10,))],
        compiler_params=pltpu.CompilerParams(vmem_limit_bytes=1024 * 1024),
    )(*results)
    return written[:4] + written[6:] + written[4:6]


def solution(mesh):
    fs_size, tp_size = mesh.shape["fs"], mesh.shape["tp"]
    placed = (
        P("fs", None),
        P("fs", "tp"),
        P("fs", "tp"),
        P("fs", None),
        P("fs", None),
        P("fs", None),
        P("fs", "tp"),
        P("tp", "fs"),
        P("fs", "tp"),
        P("fs", "tp"),
        P("fs", "tp"),
        P("fs", "tp"),
    )
    chips = fs_size // CORES
    tiled = tp_size == 2 and fs_size == 16 and chips % tp_size == 0
    return jax.shard_map(
        functools.partial(fused_body, fs_size, tp_size) if tiled else body,
        mesh=mesh,
        in_specs=placed,
        out_specs=(
            P("fs", "tp"),
            P("tp", "fs"),
            P("fs", "tp"),
            P("tp", "fs"),
            P("fs", "tp"),
            P("fs", "tp"),
            P("fs", "tp"),
            P("fs", "tp"),
            P(None, "tp"),
            P("tp", None),
        ),
        check_vma=False,
    )
```

```python
import functools

import jax
import jax.numpy as jnp
from jax import lax
from jax.experimental import pallas as pl
from jax.experimental.pallas import tpu as pltpu
from jax.sharding import PartitionSpec as P

CORES = 2

D = 2048
WIDTH = 2048


def gram_times(gram_matrix, directions):
    gram_high = gram_matrix.astype(jnp.bfloat16)
    gram_low = (gram_matrix - gram_high.astype(jnp.float32)).astype(jnp.bfloat16)
    return jnp.dot(gram_high, directions, preferred_element_type=jnp.float32) + jnp.dot(
        gram_low, directions, preferred_element_type=jnp.float32
    )


def body(
    normed_input,
    value_cotangent,
    gated_output,
    layer_cotangent,
    factor_value,
    factor_output,
    weight_value,
    weight_output,
    first_value,
    second_value,
    first_output,
    second_output,
):
    col_count = value_cotangent.shape[1]
    inner = (((0,), (0,)), ((), ()))
    pieces = (
        lax.all_gather(factor_value, "fs", axis=0, tiled=True),
        lax.all_gather(factor_output, "fs", axis=0, tiled=True),
    )
    piece_value, piece_output = pieces
    span_input = normed_input
    span_cotan = layer_cotangent
    gram_value = lax.dot_general(pieces[0], pieces[0], inner, preferred_element_type=jnp.float32)
    gram_output = lax.dot_general(pieces[1], pieces[1], inner, preferred_element_type=jnp.float32)
    projected_input = jnp.dot(span_input, piece_value, preferred_element_type=jnp.float32).astype(
        jnp.bfloat16
    )
    projected_cotangent = jnp.dot(
        span_cotan, piece_output, preferred_element_type=jnp.float32
    ).astype(jnp.bfloat16)
    span_input = projected_input
    span_cotan = projected_cotangent
    term_value = lax.dot_general(
        span_input, value_cotangent, inner, preferred_element_type=jnp.float32
    )
    term_output = lax.dot_general(
        span_cotan, gated_output, inner, preferred_element_type=jnp.float32
    )
    low_rank = lax.psum_scatter(
        jnp.concatenate([term_value, term_output], axis=1), "fs", scatter_dimension=0, tiled=True
    )
    low_value = low_rank[:, :col_count]
    low_output = low_rank[:, col_count:]
    next_first_value = 0.9 * first_value + 0.1 * low_value
    next_second_value = 0.95 * second_value + 0.05 * low_value * low_value
    next_first_output = 0.9 * first_output + 0.1 * low_output
    next_second_output = 0.95 * second_output + 0.05 * low_output * low_output
    direction_value = (next_first_value * lax.rsqrt(next_second_value)).astype(jnp.bfloat16)
    direction_output = (next_first_output * lax.rsqrt(next_second_output)).astype(jnp.bfloat16)
    gathered_value, gathered_output = (
        lax.all_gather(direction_value, "fs", axis=0, tiled=True),
        lax.all_gather(direction_output, "fs", axis=0, tiled=True),
    )
    update_value = jnp.dot(factor_value, gathered_value, preferred_element_type=jnp.float32)
    update_output = lax.dot_general(
        gathered_output, factor_output, (((0,), (1,)), ((), ())), preferred_element_type=jnp.float32
    )
    square_value = jnp.sum(
        gathered_value.astype(jnp.float32) * gram_times(gram_value, gathered_value)
    )
    square_output = jnp.sum(
        gathered_output.astype(jnp.float32) * gram_times(gram_output, gathered_output)
    )
    total_value, total_output = lax.psum((square_value, square_output), "tp")
    entries = D * WIDTH
    step_value = update_value * lax.rsqrt(total_value / entries + 1e-06)
    step_output = update_output * lax.rsqrt(total_output / entries + 1e-06)
    next_weight_value = weight_value - 0.02 * step_value
    next_weight_output = weight_output - 0.02 * step_output
    half_value = next_weight_value.astype(jnp.bfloat16)
    half_output = next_weight_output.astype(jnp.bfloat16)
    copy_value, copy_output = (
        lax.all_gather(half_value, "fs", axis=0, tiled=True),
        lax.all_gather(half_output, "fs", axis=1, tiled=True),
    )
    return (
        step_value,
        step_output,
        next_weight_value,
        next_weight_output,
        next_first_value,
        next_second_value,
        next_first_output,
        next_second_output,
        copy_value,
        copy_output,
    )


def next_moments(first, second, low):
    return 0.9 * first + 0.1 * low, 0.95 * second + 0.05 * low * low


MESH = pl.DeviceIdType.MESH


class Sender:
    def __init__(self, sems):
        self.sems, self.pending, self.drained = sems, [], 0

    def send(self, source, target, recv_sem, device, when=None):
        slots = self.sems.shape[0]
        self.drain(len(self.pending) + 1 - slots)
        copy = pltpu.make_async_remote_copy(
            src_ref=source,
            dst_ref=target,
            send_sem=self.sems.at[len(self.pending) % slots],
            recv_sem=recv_sem,
            device_id=device,
            device_id_type=MESH,
        )
        self.guarded(copy.start, when)
        self.pending.append((copy, when))

    def guarded(self, action, when):
        if when is None:
            action()
        else:

            @pl.when(when)
            def _():
                action()

    def drain(self, count=None):
        count = max(len(self.pending) if count is None else count, self.drained)
        for copy, when in self.pending[self.drained : count]:
            self.guarded(copy.wait_send, when)
        self.drained = count


def fused(
    fs_size,
    tp_size,
    input_hbm,
    value_hbm,
    gated_hbm,
    layer_hbm,
    factor_value_hbm,
    factor_output_hbm,
    weight_value_hbm,
    weight_output_hbm,
    first_value_hbm,
    second_value_hbm,
    first_output_hbm,
    second_output_hbm,
    moments,
    step_value,
    step_output,
    next_value,
    next_output,
    final_value,
    final_output,
    directions,
    turned,
    factors,
    wide_value,
    wide_output,
    stream,
    cotan,
    weight_value,
    weight_output,
    old,
    flipped,
    out_x,
    in_x,
    out_z,
    in_z,
    squares,
    totals,
    update_value,
    update_output,
    load_sem,
    send_sem,
    factor_recv,
    weight_recv,
    core_recv,
    direction_recv,
    join_recv,
    pair_recv,
    x_recv,
    z_recv,
    total_recv,
):
    fs, tp = lax.axis_index("fs"), lax.axis_index("tp")
    width = tp_size
    chips = fs_size // CORES
    depth = chips // width
    core, chip = lax.rem(fs, CORES), fs // CORES
    x, z = lax.rem(chip, width), chip // width
    rows, rank = factor_value_hbm.shape
    tokens = input_hbm.shape[0]
    cols = value_hbm.shape[1]
    ranks = first_value_hbm.shape[0]
    model = rows * fs_size
    last = depth - 1
    span = CORES * rows

    def index(z_at, x_at, core_at):
        return (z_at * width + x_at) * CORES + core_at

    def along_z(z_at):
        return {"fs": index(z_at, x, core)}

    over_x = {"fs": index(z, 1 - x, core)}
    over_core = {"fs": index(z, x, 1 - core)}
    over_y = {"tp": 1 - tp}
    diagonal = {**over_core, **over_y}
    beside = z + 1 - 2 * lax.rem(z, 2)
    mirror = last - z
    across = lax.rem(z + depth // 2, depth)
    others = (beside, mirror, across)
    middle = jnp.logical_and(z > 0, z < last)

    barrier = pltpu.get_barrier_semaphore()
    peers = [along_z(z_at) for z_at in others] + [over_x, over_core, over_y, diagonal]
    for peer in peers:
        pl.semaphore_signal(barrier, inc=1, device_id=peer, device_id_type=MESH)
    def block(ref, origin, size):
        return ref.at[pl.ds(pl.multiple_of(origin * size, size), size)]

    sources = (
        factor_value_hbm,
        factor_output_hbm,
        weight_value_hbm,
        weight_output_hbm,
        input_hbm,
        layer_hbm,
        value_hbm,
        gated_hbm,
        first_value_hbm,
        second_value_hbm,
        first_output_hbm,
        second_output_hbm,
    )
    targets = (
        block(factors.at[0], fs, rows),
        block(factors.at[1], fs, rows),
        weight_value,
        weight_output,
        stream.at[0],
        stream.at[1],
        cotan.at[0],
        cotan.at[1],
        old.at[0],
        old.at[1],
        old.at[2],
        old.at[3],
    )
    loads = [
        pltpu.make_async_copy(source, target, load_sem.at[slot])
        for slot, (source, target) in enumerate(zip(sources, targets))
    ]
    for load in loads:
        load.start()

    loads[0].wait()
    loads[1].wait()
    pl.semaphore_wait(barrier, len(peers))

    sender = Sender(send_sem)

    def projected(kind):
        return (pl.ds(0, tokens), pl.ds(pl.multiple_of(kind * rank, rank), rank))

    def term_at(to, core_at):
        start = pl.multiple_of(tokens + (to * CORES + core_at) * ranks, ranks)
        return update_output.at[pl.ds(start, ranks), pl.ds(0, 2 * cols)]

    def paired_at(to):
        start = pl.multiple_of(tokens + rank + to * ranks, ranks)
        return update_output.at[pl.ds(start, ranks), pl.ds(0, 2 * cols)]

    def arrived(ref, recv_sem):
        pltpu.make_async_remote_copy(
            src_ref=ref,
            dst_ref=ref,
            send_sem=send_sem.at[0],
            recv_sem=recv_sem,
            device_id=over_core,
            device_id_type=MESH,
        ).wait_recv()

    def forward(ref, recv_sem, device, when=None):
        sender.send(ref, ref, recv_sem, device, when)

    mine, theirs = tp, 1 - tp

    def factor(kind, origin):
        return block(factors.at[kind], origin, rows), factor_recv.at[kind, origin]

    for z_at in others:
        forward(*factor(mine, fs), along_z(z_at))
    forward(*factor(mine, fs), over_x)
    forward(*factor(theirs, fs), over_x)
    forward(*factor(mine, fs), over_core)
    forward(*factor(theirs, fs), over_core)

    direct = (1,)
    lead, half_cols = rows * 3 // 8, cols // 2

    def piece(part, origin):
        start = pl.multiple_of(origin * rows, rows)
        if part < 2:
            ref = wide_value.at[pl.ds(start + part * lead, rows - lead if part else lead)]
        else:
            ref = wide_output.at[pl.ds((part - 2) * half_cols, half_cols), pl.ds(start, rows)]
        return ref, weight_recv.at[part, origin // CORES]

    def piece_to_core(part, origin, when=None):
        ref, _ = piece(part, origin)
        forward(ref, core_recv.at[part // 2, origin // CORES], over_core, when)

    def piece_z(part, origin):
        forward(*piece(part, origin), along_z(beside))
        forward(*piece(part, origin), along_z(mirror), middle)
        if part in direct:
            forward(*piece(part, origin), along_z(across))

    def piece_from_z(part, z_at, x_at, onward, when=None):
        ref, sem = piece(part, index(z_at, x_at, core))
        sender.guarded(lambda: arrived(ref, sem), when)
        if onward is not None:
            forward(ref, sem, along_z(onward), middle)
        piece_to_core(part, index(z_at, x_at, core), when)

    def near(part, x_at):
        relayed = part not in direct
        piece_from_z(part, beside, x_at, mirror if relayed else None)
        piece_from_z(part, mirror, x_at, beside if relayed else None, middle)

    def second(part, x_at):
        piece_from_z(part, across, x_at, beside)

    def third(part, x_at):
        piece_from_z(part, mirror, x_at, None, jnp.logical_not(middle))

    def cross(part, *z_ats):
        for z_at in z_ats:
            forward(*piece(part, index(z_at, x, core)), over_x)

    def to_core(part, *z_ats):
        for z_at in z_ats:
            piece_to_core(part, index(z_at, x, core))

    def from_x(part, *z_ats):
        for z_at in z_ats:
            arrived(*piece(part, index(z_at, 1 - x, core)))
            piece_to_core(part, index(z_at, 1 - x, core))

    loads[2].wait()
    loads[3].wait()
    own_rows = pl.ds(pl.multiple_of(fs * rows, rows), rows)
    wide_value[own_rows, :] = weight_value[...].astype(jnp.bfloat16)
    wide_output[:, own_rows] = weight_output[...].astype(jnp.bfloat16)
    cross(0, z)
    piece_z(1, fs)
    piece_z(2, fs)
    piece_z(3, fs)

    for z_at in others:
        ref, sem = factor(mine, index(z_at, x, core))
        arrived(ref, sem)
        forward(ref, sem, over_x)
        forward(ref, sem, over_y)
        forward(ref, sem, over_core)
    for part in (1, 2, 3):
        cross(part, z)
    ref, sem = factor(theirs, index(z, 1 - x, core))
    arrived(ref, sem)
    forward(ref, sem, over_core)
    for z_at in (z,) + others:
        ref, sem = factor(mine, index(z_at, 1 - x, core))
        arrived(ref, sem)
        if z_at is not z:
            forward(ref, sem, over_y)
        forward(ref, sem, over_core)
    for load in loads[4:]:
        load.wait()

    def project(kind, z_at, x_at, first=False):
        arrived(*factor(kind, index(z_at, x_at, 1 - core)))
        part = pl.ds(pl.multiple_of((z_at * width + x_at) * span, span), span)
        product = jnp.dot(
            stream[kind, :, part], factors[kind, part], preferred_element_type=jnp.float32
        )
        at = projected(kind)
        update_output[at] = product if first else update_output[at] + product

    def from_y(z_at, x_at):
        ref, sem = factor(theirs, index(z_at, x_at, core))
        arrived(ref, sem)
        forward(ref, sem, over_core)

    project(mine, z, x, True)
    project(theirs, z, x, True)
    for z_at in others:
        project(mine, z_at, x)
    for z_at in others:
        from_y(z_at, x)
    for z_at in (z,) + others:
        project(mine, z_at, 1 - x)
    for z_at in others:
        from_y(z_at, 1 - x)
    width_tile = 256

    def terms_of(kind):
        flipped[...] = update_output[projected(kind)].T.astype(jnp.bfloat16)

        @pl.loop(0, cols // width_tile)
        def _(step):
            tile = pl.ds(pl.multiple_of(step * width_tile, width_tile), width_tile)
            term = jnp.dot(flipped[...], cotan[kind, :, tile], preferred_element_type=jnp.float32)
            start = pl.multiple_of(kind * cols + step * width_tile, width_tile)
            update_output[tokens : tokens + rank, pl.ds(start, width_tile)] = term

    for part in range(4):
        to_core(part, z)
    near(1, x)
    terms_of(mine)
    for z_at in others:
        project(theirs, z_at, x)
    for z_at in (z,) + others:
        project(theirs, z_at, 1 - x)

    second(1, x)
    cross(1, beside)
    terms_of(theirs)

    far = others + (z,)
    for x_at in (1 - x, x):
        for z_at in far:
            to = z_at * width + x_at
            sender.send(term_at(to, 1 - core), paired_at(to), pair_recv.at[to], over_core)

    def pair_sum(z_at, x_at):
        at = z_at * width + x_at
        arrived(paired_at(at), pair_recv.at[at])
        return term_at(at, core)[...] + paired_at(at)[...]

    for z_at in far:
        out_x[z_at] = pair_sum(z_at, 1 - x).astype(jnp.bfloat16)
        sender.send(out_x.at[z_at], in_x.at[z_at], x_recv.at[z_at], over_x)
    near(2, x)
    cross(1, across)
    near(3, x)
    from_x(0, z)

    def column_sum(z_at):
        total = pair_sum(z_at, x)
        arrived(in_x.at[z_at], x_recv.at[z_at])
        return total + in_x[z_at].astype(jnp.float32)

    for z_at in others:
        out_z[z_at] = column_sum(z_at).astype(jnp.bfloat16)
        sender.send(out_z.at[z_at], in_z.at[z], z_recv.at[z], along_z(z_at))
    early = len(sender.pending)
    low = column_sum(z)
    cross(2, beside)
    second(2, x)
    for part in (1, 2, 3):
        from_x(part, z)
    for z_at in others:
        arrived(in_z.at[z_at], z_recv.at[z_at])
        low = low + in_z[z_at].astype(jnp.float32)

    own_ranks = pl.ds(pl.multiple_of(fs * ranks, ranks), ranks)
    for kind in range(2):
        part = low[:, kind * cols : (kind + 1) * cols]
        next_first, next_second = next_moments(old[2 * kind], old[2 * kind + 1], part)
        moments[2 * kind] = next_first
        moments[2 * kind + 1] = next_second
        directions[own_ranks, kind * cols : (kind + 1) * cols] = (
            next_first * lax.rsqrt(next_second)
        ).astype(jnp.bfloat16)

    def direction(origin):
        return block(directions, origin, ranks), direction_recv.at[origin // CORES]

    for z_at in others:
        forward(*direction(fs), along_z(z_at))
    forward(*direction(fs), over_x)
    forward(direction(fs)[0], join_recv.at[0], over_core)
    cross(3, beside)
    piece_z(0, fs)
    second(3, x)
    piece_z(0, index(z, 1 - x, core))
    for z_at in others:
        ref, sem = direction(index(z_at, x, core))
        arrived(ref, sem)
        forward(ref, sem, over_x)
        forward(ref, join_recv.at[0], over_core)
    cross(2, across)
    third(1, x)
    cross(1, mirror)
    from_x(1, beside, across)
    for z_at in (z,) + others:
        ref, sem = direction(index(z_at, 1 - x, core))
        arrived(ref, sem)
        forward(ref, join_recv.at[0], over_core)
    near(0, x)
    cross(3, across)
    third(2, x)
    cross(2, mirror)
    arrived(directions.at[pl.ds(0, chips * ranks)], join_recv.at[0])
    half = chips // CORES
    me = tp * CORES + core

    def updates(kind, side, counted):
        if counted:
            squares[kind] = jnp.zeros((8, cols), jnp.float32)

        @pl.loop(0, half)
        def _(step):
            part = pl.ds(pl.multiple_of((side * half + step) * span, span), span)
            if kind == 0:
                update = jnp.dot(
                    factors[0, part], directions[:, :cols], preferred_element_type=jnp.float32
                )
                update_value[part] = update
            else:
                update = lax.dot_general(
                    turned[...],
                    factors[1, part],
                    (((1,), (1,)), ((), ())),
                    preferred_element_type=jnp.float32,
                )
                update_output[:, part] = update
            if counted:
                square = update * update
                lanes = square.shape[1]
                squares[kind, :, :lanes] += jnp.sum(square.reshape(-1, 8, lanes), axis=0)

        if counted:
            folded = squares[kind, :, :128]
            for lane in range(128, cols, 128):
                folded = folded + squares[kind, :, lane : lane + 128]
            totals[me, kind] = folded

    sender.drain(early)
    updates(0, core, True)
    near(0, 1 - x)
    turned[...] = directions[:, cols:].astype(jnp.float32).T.astype(jnp.bfloat16)
    second(0, x)
    third(3, x)
    cross(3, mirror)
    updates(1, core, True)
    for device in (over_y, over_core, diagonal):
        sender.send(totals.at[me], totals.at[me], total_recv.at[me], device)
    second(0, 1 - x)
    updates(0, 1 - core, False)
    updates(1, 1 - core, False)
    from_x(1, mirror)
    from_x(2, beside, across)
    from_x(3, beside)
    for tp_at, core_at in ((tp, 1 - core), (1 - tp, core), (1 - tp, 1 - core)):
        slot = tp_at * CORES + core_at
        arrived(totals.at[slot], total_recv.at[slot])
    entries = model * cols * tp_size
    scales = [
        lax.rsqrt(jnp.sum(jnp.sum(totals[:, kind], axis=0), keepdims=True) / entries + 1e-06)
        for kind in range(2)
    ]
    def finals(kind, z_at, x_at):
        at = z_at * width + x_at
        sent = pl.ds(pl.multiple_of((at * CORES + 1 - core) * rows, rows), rows)
        arrived((wide_output.at[:, sent] if kind else wide_value.at[sent]), core_recv.at[kind, at])
        part = pl.ds(pl.multiple_of((z_at * width + x_at) * span, span), span)
        scale = 0.02 * scales[kind]
        if kind == 0:
            final_value[part] = (
                wide_value[part].astype(jnp.float32) - update_value[part] * scale
            ).astype(jnp.bfloat16)
        else:
            final_output[:, part] = (
                wide_output[:, part].astype(jnp.float32) - update_output[:, part] * scale
            ).astype(jnp.bfloat16)

    step = update_value[own_rows] * scales[0]
    step_value[...] = step
    next_value[...] = weight_value[...] - 0.02 * step
    step = update_output[:, own_rows] * scales[1]
    step_output[...] = step
    next_output[...] = weight_output[...] - 0.02 * step
    finals(0, z, x)
    finals(1, z, x)
    finals(1, beside, x)
    from_x(3, across)
    third(0, x)
    finals(0, beside, x)
    finals(0, across, x)
    finals(1, across, x)
    from_x(2, mirror)
    finals(1, z, 1 - x)
    third(0, 1 - x)
    for z_at in (z, beside, across):
        finals(0, z_at, 1 - x)
    finals(1, beside, 1 - x)
    from_x(3, mirror)
    finals(0, mirror, x)
    finals(1, mirror, x)
    finals(0, mirror, 1 - x)
    finals(1, across, 1 - x)
    finals(1, mirror, 1 - x)
    sender.drain()


def write(count, *refs):
    sems = refs[-1]
    sources = refs[5:count] + refs[1:5] + tuple(refs[0].at[k] for k in range(4))
    targets = refs[count + 4 : count + 6] + refs[count : count + 4] + refs[count + 6 : -1]
    copies = [
        pltpu.make_async_copy(source, target, sems.at[slot])
        for slot, (source, target) in enumerate(zip(sources, targets))
    ]
    for copy in copies:
        copy.start()
    for copy in copies:
        copy.wait()


def fused_body(fs_size, tp_size, *args):
    tokens, model = args[0].shape
    cols = args[1].shape[1]
    rows, rank = args[4].shape
    ranks = args[8].shape[0]
    chips = fs_size // CORES
    depth = chips // tp_size
    f32, bf16 = jnp.float32, jnp.bfloat16
    vmem = pl.BlockSpec(memory_space=pltpu.VMEM)
    hbm = pl.BlockSpec(memory_space=pltpu.HBM)
    shape = jax.ShapeDtypeStruct
    dma = pltpu.SemaphoreType.DMA
    args = [pltpu.with_memory_space_constraint(arg, pltpu.HBM) for arg in args]
    own = [shape((rows, cols), f32), shape((cols, rows), f32)] * 2
    copies = [shape((model, cols), bf16), shape((cols, model), bf16)]
    results = pl.pallas_call(
        functools.partial(fused, fs_size, tp_size),
        out_shape=[shape((4, ranks, cols), f32)] + own + copies,
        in_specs=[hbm] * 12,
        out_specs=[vmem] * 7,
        scratch_shapes=[
            pltpu.VMEM((rank, 2 * cols), bf16),
            pltpu.VMEM((cols, rank), bf16),
            pltpu.VMEM((2, model, rank), bf16),
            pltpu.VMEM((model, cols), bf16),
            pltpu.VMEM((cols, model), bf16),
            pltpu.VMEM((2, tokens, model), bf16),
            pltpu.VMEM((2, tokens, cols), bf16),
            pltpu.VMEM((rows, cols), f32),
            pltpu.VMEM((cols, rows), f32),
            pltpu.VMEM((4, ranks, cols), f32),
            pltpu.VMEM((rank, tokens), bf16),
        ]
        + [pltpu.VMEM((depth, ranks, 2 * cols), bf16)] * 4
        + [
            pltpu.VMEM((2, 8, cols), f32),
            pltpu.VMEM((tp_size * CORES, 2, 8, 128), f32),
            pltpu.VMEM((model, cols), f32),
            pltpu.VMEM((cols, model), f32),
            dma((12,)),
            dma((40,)),
            dma((2, fs_size)),
            dma((4, chips)),
            dma((2, chips)),
            dma((chips,)),
            dma((1,)),
            dma((chips,)),
            dma((depth,)),
            dma((depth,)),
            dma((tp_size * CORES,)),
        ],
        compiler_params=pltpu.CompilerParams(
            collective_id=0, has_side_effects=True, vmem_limit_bytes=40 * 1024 * 1024
        ),
    )(*args)

    written = pl.pallas_call(
        functools.partial(write, len(results)),
        out_shape=own + copies + [shape((ranks, cols), f32)] * 4,
        in_specs=[vmem] * len(results),
        out_specs=[hbm] * 10,
        scratch_shapes=[dma((10,))],
        compiler_params=pltpu.CompilerParams(vmem_limit_bytes=1024 * 1024),
    )(*results)
    return written[:4] + written[6:] + written[4:6]


def solution(mesh):
    fs_size, tp_size = mesh.shape["fs"], mesh.shape["tp"]
    placed = (
        P("fs", None),
        P("fs", "tp"),
        P("fs", "tp"),
        P("fs", None),
        P("fs", None),
        P("fs", None),
        P("fs", "tp"),
        P("tp", "fs"),
        P("fs", "tp"),
        P("fs", "tp"),
        P("fs", "tp"),
        P("fs", "tp"),
    )
    chips = fs_size // CORES
    tiled = tp_size == 2 and fs_size == 16 and chips % tp_size == 0
    return jax.shard_map(
        functools.partial(fused_body, fs_size, tp_size) if tiled else body,
        mesh=mesh,
        in_specs=placed,
        out_specs=(
            P("fs", "tp"),
            P("tp", "fs"),
            P("fs", "tp"),
            P("tp", "fs"),
            P("fs", "tp"),
            P("fs", "tp"),
            P("fs", "tp"),
            P("fs", "tp"),
            P(None, "tp"),
            P("tp", None),
        ),
        check_vma=False,
    )
```
